256 devices in a mesh: grp: 2 (over z), ep: 64 (over y, x), tp: 2 (over core).
Axes of the slice: x: 8, y: 8, z: 2, core: 2. Of those that a mesh axis runs over, the one named last changes fastest.
The devices are a block of a 8x8x16 slice.
Arguments:
- tokens: bfloat16 [8192, 1024], P(('grp', 'ep')), parts along dimension 0, may hold values from -6 to 6
- routes: int32 [8192, 4], P(('grp', 'ep')), parts along dimension 0, may hold values from 0 to 63, all different within a row; in each aligned block of 64 rows (0 to 63, 64 to 127, ...) at most 12 rows name the same one
- gates: float32 [8192, 4], P(('grp', 'ep')), parts along dimension 0, may hold values from 0.05 to 1
- norm_gain: float32 [1024], replicated, may hold values from 0.1 to 1.9
- w_gate: bfloat16 [64, 1024, 1792], P('ep', None, 'tp'), may hold values from -0.1875 to 0.1875
- w_up: bfloat16 [64, 1024, 1792], P('ep', None, 'tp'), may hold values from -0.1875 to 0.1875
- w_down: bfloat16 [64, 1792, 1024], P('ep', 'tp'), may hold values from -0.125 to 0.125
Outputs:
- mixed: bfloat16 [8192, 1024], P(('grp', 'ep')), parts along dimension 0
The draws below stay inside these ranges and needn't reach their ends.
There are 2 independent parts, one for each index of `grp`. The reference program is written for one: setup_inputs(seed, part) draws one part's arguments, and reference() takes and returns one part's arrays. A program takes and returns all parts, laid end to end along the dimension named above; an argument that names none is the same for every part. Nothing has to cross between parts.
Inputs may be any that keep to these rules, and one draw needn't show every extreme that they name: `routes`: within the rows of one index of ep no expert is named more than 12 times; some expert is named exactly 12 times there in some or all of them.
All inputs are finite; a program needn't handle non-finite values.
Results may differ from the reference program's by a relative error of at most 0.0078.
Values may be sent and summed in bfloat16 or wider, within the bound.
No kernel may reach another device: no remote copies, remote signals or barrier semaphores. Data moves between devices by JAX's collectives and lax.ppermute only.
A program may use at most 64 MiB of HBM per device.

```python
import math
import jax
import jax.numpy as jnp
import numpy as np
from jax import lax

D = 1024
FF = 1792
TOP_K = 4
TOK_DEV = 64
EXPERTS = 64
CAP = 12
TOKENS = 4096
N_EP = 64
N_TP = 2


def steps_of(own_key, extent, pieces, low, high):
    factor_of = 1.0
    for axis_at, parts in pieces:
        heights = jax.random.uniform(jax.random.fold_in(jax.random.fold_in(own_key, 6), axis_at), (parts,), jnp.float32, low / len(pieces), high / len(pieces))
        factor_of = factor_of * jnp.repeat(jnp.exp(heights), extent[axis_at] // parts).reshape((-1,) + (1,) * (len(extent) - 1 - axis_at))
    return factor_of


def deal_out(rng, own, number, rows, count, top, bound, lean):
    ranking = jax.random.permutation(rng, count)
    packed, ordinary = shares(count, rows * top, bound, lean, True), shares(count, rows * top, bound, lean, False)
    places = jnp.arange(count)

    def named(lengths, turn):
        used = int((lengths > 0).sum())
        fixed = max(1, used // 4)
        shifted = fixed + (places - fixed + turn * (used - fixed)) % max(1, count - fixed)
        return jnp.zeros((count,), jnp.int32).at[ranking[jnp.where(places < fixed, places, shifted)]].set(jnp.asarray(lengths, jnp.int32))

    lengths = jnp.where(number % 4 == 0, named(packed, number // 4), named(ordinary, number - number // 4 - 1))
    mixed = jax.random.permutation(jax.random.fold_in(own, 3), count)
    donor, taker = mixed[0:count // 2 * 2:2], mixed[1:count // 2 * 2:2]
    room = jnp.minimum(lengths[donor] - 1, bound - lengths[taker]) // 2
    room = jnp.where((donor == ranking[0]) | (taker == ranking[0]) | (lengths[taker] == 0), 0, jnp.maximum(room, 0))
    shifted = jax.random.randint(jax.random.fold_in(own, 4), (count // 2,), 0, 1 << 20) % (room + 1)
    lengths = lengths.at[donor].add(-shifted).at[taker].add(shifted)
    members = jnp.searchsorted(jnp.cumsum(lengths), jnp.arange(rows * top), side="right").astype(jnp.int32)
    grid = members.reshape(top, rows).T
    grid = grid[jax.random.permutation(jax.random.fold_in(own, 1), rows)]
    turn = jax.random.randint(jax.random.fold_in(own, 2), (rows, 1), 0, top)
    return jnp.take_along_axis(grid, (jnp.arange(top)[None, :] + turn) % top, axis=1)


def shares(number_of, total, limit, skew, full):
    portions = [(1 << 20) // math.isqrt(rank ** skew) + 1 for rank in range(1, number_of + 1)]
    largest = limit if full else min(limit, max(-(-total // number_of), total * portions[0] // sum(portions)))
    least = 1 if total - largest >= number_of - 1 else 0
    given, rest = [largest] + [least] * (number_of - 1), total - largest - least * (number_of - 1)
    while rest > 0:
        movable = [i for i in range(1, number_of) if given[i] < largest] or [i for i in range(1, number_of) if given[i] < limit]
        mass, left = sum([portions[i] for i in movable]), rest
        for i in movable:
            extra = min(limit - given[i], max(1, left * portions[i] // mass), rest)
            given[i] = given[i] + extra
            rest = rest - extra
    return np.array(given)


def noise(key, extent, scale, bound, cuts=(), kind=jnp.bfloat16):
    entries = scale * jax.random.normal(key, extent, jnp.float32)
    if cuts:
        entries = entries * steps_of(key, extent, cuts, -0.22, 0.18)
    return jnp.clip(entries, -bound, bound).astype(kind)


def setup_inputs(seed: int = 0, part: int = 0) -> dict:
    streams_of = jax.random.split(jax.random.key(seed), 8)
    part_splits = jax.random.split(jax.random.fold_in(streams_of[7], part), 8)
    tokens = noise(part_splits[0], (TOKENS, D), 1.0, 6.0, ((0, 64),))
    routes_keys = jax.random.split(jax.random.fold_in(part_splits[1], 1), TOKENS // TOK_DEV)
    routes_turns = jax.random.permutation(jax.random.fold_in(part_splits[1], 3), TOKENS // TOK_DEV)
    routes = jax.vmap(lambda own, number: deal_out(jax.random.fold_in(part_splits[1], 2), own, number, TOK_DEV, EXPERTS, TOP_K, CAP, 2))(routes_keys, routes_turns).reshape((TOKENS, TOP_K))
    gates = jnp.clip(0.05 + 0.95 * jax.random.uniform(part_splits[2], (TOKENS, TOP_K), jnp.float32) ** steps_of(part_splits[2], (TOKENS, TOP_K), ((0, 64),), -0.2, 0.2), 0.05, 1.0)
    norm_gain = jnp.clip(1.0 + 0.18 * jax.random.normal(streams_of[3], (D,), jnp.float32), 0.1, 1.9)
    w_gate = noise(streams_of[4], (EXPERTS, D, FF), D ** -0.5, 0.1875, ((0, 64), (2, 2)))
    w_up = noise(streams_of[5], (EXPERTS, D, FF), D ** -0.5, 0.1875, ((0, 64), (2, 2)))
    w_down = noise(streams_of[6], (EXPERTS, FF, D), FF ** -0.5, 0.125, ((0, 64), (1, 2)))
    return {"tokens": tokens, "routes": routes, "gates": gates, "norm_gain": norm_gain, "w_gate": w_gate, "w_up": w_up, "w_down": w_down}


EPS = 1e-06

def reference(tokens, routes, gates, norm_gain, w_gate, w_up, w_down):
    xf = tokens.astype(jnp.float32)
    normed = (xf * lax.rsqrt(lax.optimization_barrier(jnp.mean(xf * xf, axis=-1, keepdims=True)) + EPS) * norm_gain.astype(jnp.float32)).astype(jnp.bfloat16)
    flat = routes.reshape(-1).astype(jnp.int32)
    pair_count = TOKENS * TOP_K
    rows_max = N_EP * CAP
    block = FF // N_TP

    def expert(index):
        chosen = jnp.nonzero(flat == index, size=rows_max, fill_value=pair_count)[0].astype(jnp.int32)
        source = jnp.minimum(chosen // TOP_K, TOKENS - 1).astype(jnp.int32)
        picked = jnp.take(normed, source, axis=0)
        gate_act = jnp.dot(picked, w_gate[index], preferred_element_type=jnp.float32)
        up_act = jnp.dot(picked, w_up[index], preferred_element_type=jnp.float32)
        hidden = (jax.nn.silu(gate_act) * up_act).astype(jnp.bfloat16)
        total = jnp.zeros((rows_max, D), jnp.float32)
        for part_index in range(N_TP):
            rows_down = w_down[index, part_index * block:(part_index + 1) * block]
            part = jnp.dot(hidden[:, part_index * block:(part_index + 1) * block], rows_down, preferred_element_type=jnp.float32).astype(jnp.bfloat16)
            total = total + lax.optimization_barrier(part).astype(jnp.float32)
        return (chosen, total.astype(jnp.bfloat16))
    chosen_all, results_all = lax.map(expert, jnp.arange(EXPERTS, dtype=jnp.int32))
    pair_out = jnp.zeros((pair_count, D), jnp.bfloat16).at[chosen_all.reshape(-1)].set(results_all.reshape(-1, D), mode='drop')
    mixed = lax.optimization_barrier(jnp.sum(gates.astype(jnp.float32)[:, :, None] * pair_out.reshape(TOKENS, TOP_K, D).astype(jnp.float32), axis=1))
    return mixed.astype(jnp.bfloat16)
```

```python
import functools

import jax
import jax.numpy as jnp
from jax import lax
from jax.experimental import pallas as pl
from jax.experimental.pallas import tpu as pltpu
from jax.sharding import PartitionSpec as P

EPS = 1e-06
BF = jnp.bfloat16
F32 = jnp.float32
VMEM = pl.BlockSpec(memory_space=pltpu.VMEM)
SMEM = pl.BlockSpec(memory_space=pltpu.SMEM)
LIMIT = 24 * 1024 * 1024


def dot(a, b):
    return jnp.dot(a, b, preferred_element_type=F32)


def iota(shape, dim):
    return lax.broadcasted_iota(jnp.int32, shape, dim)


def call(body, out_shape, n_smem, n_in, scratch=(), flops=0):
    return pl.pallas_call(
        body,
        out_shape=out_shape,
        in_specs=[SMEM] * n_smem + [VMEM] * n_in,
        out_specs=jax.tree.map(lambda _: VMEM, out_shape),
        scratch_shapes=list(scratch),
        compiler_params=pltpu.CompilerParams(vmem_limit_bytes=LIMIT),
        cost_estimate=pl.CostEstimate(flops=flops, bytes_accessed=0, transcendentals=0),
    )


def div_const(x, n):
    mul = -(-(1 << 17) // n)
    return (x * mul) >> 17


def prep_body(lane_ref, tok_ref, gain_ref, rt_ref, out_ref, half_ref, *, experts, cap):
    rows, width = tok_ref.shape
    share = width // 2
    q = share // 2
    xf = tok_ref[...].astype(F32)
    var = jnp.mean(xf * xf, axis=-1, keepdims=True)
    normed = (xf * lax.rsqrt(var + EPS) * gain_ref[...]).astype(BF)
    for c in range(2):
        for h in range(2):
            half_ref[c, h * rows : (h + 1) * rows, :] = normed[:, c * share + h * q : c * share + (h + 1) * q]
    stacked = half_ref[lane_ref[0]]
    wide = 2 * rows
    rt = rt_ref[...]
    e_of = iota((experts, wide), 0)
    chosen = jnp.zeros((experts, wide), F32)
    for k in range(rt.shape[0]):
        chosen = chosen + (e_of == rt[k : k + 1, :]).astype(F32)
    t_of = iota((wide, wide), 1)
    before = iota((wide, wide), 0)
    upper = jnp.where(before < jnp.where(t_of >= rows, t_of - rows, t_of), 1.0, 0.0)
    upper = jnp.where(before < rows, upper, 0.0).astype(BF)
    rank = dot(chosen.astype(BF), upper)
    place = jnp.where(chosen > 0, rank, -1.0).astype(BF)
    group = 8
    block = group * 2 * cap
    r = iota((block, wide), 0)
    e_in = div_const(r, 2 * cap)
    left = r - e_in * (2 * cap)
    h_in = (left >= cap).astype(jnp.int32)
    slot = (left - h_in * cap).astype(F32)
    right_half = h_in == (iota((block, wide), 1) >= rows).astype(jnp.int32)
    e_row = div_const(iota((block, experts), 0), 2 * cap)
    e_col = iota((block, experts), 1)
    for b in range(experts // group):
        rep = (e_col == e_row + b * group).astype(F32).astype(BF)
        ranks = dot(rep, place)
        one = jnp.where((ranks == slot) & right_half, 1.0, 0.0).astype(BF)
        out_ref[b * block : (b + 1) * block, :] = dot(one, stacked).astype(BF)


def sort_matrix(cap, group, transposed):
    n = group * 2 * cap
    half = group * cap
    qdim, pdim = (1, 0) if transposed else (0, 1)
    qq = iota((n, n), qdim)
    h = (qq >= half).astype(jnp.int32)
    i = qq - h * half
    b = div_const(i, cap)
    src = b * (2 * cap) + h * cap + (i - b * cap)
    return jnp.where(iota((n, n), pdim) == src, 1.0, 0.0).astype(BF)


def unpack(x_ref, rows_ref, cap, group):
    n = group * 2 * cap
    half = n // 2
    q = x_ref.shape[1]
    perm = sort_matrix(cap, group, False)
    for b in range(x_ref.shape[0] // n):
        got = dot(perm, x_ref[b * n : (b + 1) * n, :]).astype(BF)
        for h in range(2):
            rows_ref[b * half : (b + 1) * half, h * q : (h + 1) * q] = got[h * half : (h + 1) * half, :]


def pack(y, out_ref, cap, group):
    n = group * 2 * cap
    half = n // 2
    q = y.shape[1] // 2
    perm = sort_matrix(cap, group, True)
    for b in range(y.shape[0] // half):
        part = y[b * half : (b + 1) * half]
        stacked = jnp.concatenate([part[:, :q], part[:, q:]], axis=0)
        out_ref[b * n : (b + 1) * n, :] = dot(perm, stacked).astype(BF)


def first_body(lane_ref, x_ref, wg_ref, wu_ref, acc_ref, rows_ref, *, cap, group):
    share = rows_ref.shape[1]
    unpack(x_ref, rows_ref, cap, group)
    start = pl.multiple_of(lane_ref[0] * share, share)
    rows = rows_ref[...]
    for n in range(acc_ref.shape[0]):
        cols = slice(n * 128, (n + 1) * 128)
        w = jnp.concatenate([wg_ref[pl.ds(start, share), cols], wu_ref[pl.ds(start, share), cols]], axis=1)
        acc_ref[n] = dot(rows, w)


def second_body(lane_ref, x_ref, wg_ref, wu_ref, wd_ref, acc_ref, hid_ref, out_ref, rows_ref, *, cap, group):
    share = rows_ref.shape[1]
    unpack(x_ref, rows_ref, cap, group)
    start = pl.multiple_of((1 - lane_ref[0]) * share, share)
    rows = rows_ref[...]
    for n in range(acc_ref.shape[0]):
        cols = slice(n * 128, (n + 1) * 128)
        w = jnp.concatenate([wg_ref[pl.ds(start, share), cols], wu_ref[pl.ds(start, share), cols]], axis=1)
        both = acc_ref[n] + dot(rows, w)
        g, u = both[:, :128], both[:, 128:]
        hid_ref[:, cols] = (g / (1.0 + jnp.exp(-g)) * u).astype(BF)
    y = dot(hid_ref[...], wd_ref[:, pl.ds(start, share)]).astype(BF)
    pack(y, out_ref, cap, group)


def third_body(lane_ref, hid_ref, wd_ref, rt_ref, gt_ref, out_ref, mix_ref, *, cap, group, experts):
    share = wd_ref.shape[1] // 2
    start = pl.multiple_of(lane_ref[0] * share, share)
    y = dot(hid_ref[...], wd_ref[:, pl.ds(start, share)]).astype(BF)
    pack(y, out_ref, cap, group)
    toks, top = rt_ref.shape
    e_of = iota((toks, experts), 1)
    chosen = jnp.zeros((toks, experts), F32)
    gate = jnp.zeros((toks, experts), F32)
    for k in range(top):
        hit = e_of == rt_ref[:, k : k + 1]
        chosen = chosen + hit.astype(F32)
        gate = gate + jnp.where(hit, gt_ref[:, k : k + 1], 0.0)
    lower = (iota((toks, toks), 1) < iota((toks, toks), 0)).astype(F32).astype(BF)
    rank = dot(lower, chosen.astype(BF))
    place = jnp.where(chosen > 0, rank, -1.0).astype(BF)
    g1 = gate.astype(BF)
    rest = gate - g1.astype(F32)
    g2 = rest.astype(BF)
    g3 = (rest - g2.astype(F32)).astype(BF)
    tall = jnp.concatenate([place, g1, g2, g3], axis=0)
    n = 2 * cap * experts
    r = iota((1, n), 1)
    e_r = div_const(r, 2 * cap)
    left = r - e_r * (2 * cap)
    h_r = left >= cap
    slot = jnp.where(h_r, left - cap, left).astype(F32)
    rep = (iota((experts, n), 0) == e_r).astype(F32).astype(BF)
    spread = dot(tall, rep)
    here = spread[:toks] == slot
    for h in range(2):
        ok = here & (h_r if h else jnp.logical_not(h_r))
        for i in range(3):
            piece = spread[(1 + i) * toks : (2 + i) * toks]
            at = (h * 3 + i) * toks
            mix_ref[at : at + toks, :] = jnp.where(ok, piece, 0.0).astype(BF)


def last_body(mix_ref, back_ref, out_ref):
    toks = out_ref.shape[0]
    q = back_ref.shape[1]
    s = dot(mix_ref[...], back_ref[...])
    for h in range(2):
        at = 3 * h * toks
        total = s[at : at + toks] + s[at + toks : at + 2 * toks] + s[at + 2 * toks : at + 3 * toks]
        out_ref[:, h * q : (h + 1) * q] = total.astype(BF)


def per_device(tokens, routes, gates, norm_gain, w_gate, w_up, w_down):
    toks, width = tokens.shape
    top = routes.shape[1]
    experts = lax.axis_size("ep")
    cap = max(2, min(toks, 3 * toks * top // experts))
    share = width // 2
    q = share // 2
    ff = w_gate.shape[2]
    items = experts * cap
    group = 8
    swap = lambda v: lax.ppermute(v, "tp", [(0, 1), (1, 0)])
    lane = lax.axis_index("tp").astype(jnp.int32)
    lanes = lane.reshape(1)
    rt = routes.T
    rt2 = jnp.concatenate([rt, rt], axis=1)
    struct = jax.ShapeDtypeStruct
    wide = struct((2 * items, q), BF)

    outgoing = call(
        functools.partial(prep_body, experts=experts, cap=cap), wide, 1, 3,
        [pltpu.VMEM((2, 2 * toks, q), BF)], flops=2 * 2 * items * 2 * toks * q,
    )(lanes, tokens, norm_gain.reshape(1, width), rt2)
    exchange = lambda v: lax.all_to_all(
        v.reshape(experts, 2 * cap, q), "ep", split_axis=0, concat_axis=0, tiled=True
    ).reshape(2 * items, q)
    mine = exchange(outgoing)
    other = swap(mine)
    wg, wu, wd = w_gate[0], w_up[0], w_down[0]
    blocks = ff // 128
    acc = call(
        functools.partial(first_body, cap=cap, group=group), struct((blocks, items, 256), F32), 1, 3,
        [pltpu.VMEM((items, share), BF)], flops=2 * items * share * 2 * ff,
    )(lanes, mine, wg, wu)
    hidden, sent = call(
        functools.partial(second_body, cap=cap, group=group), (struct((items, ff), BF), wide), 1, 5,
        [pltpu.VMEM((items, share), BF)], flops=2 * items * share * 3 * ff,
    )(lanes, other, wg, wu, wd, acc)
    got = swap(sent)
    kept, table = call(
        functools.partial(third_body, cap=cap, group=group, experts=experts),
        (wide, struct((6 * toks, 2 * items), BF)), 1, 4, flops=2 * items * share * ff,
    )(lanes, hidden, wd, routes, gates)
    results = (kept.astype(F32) + got.astype(F32)).astype(BF)
    back = exchange(results)
    part = call(last_body, struct((toks, share), BF), 0, 2, flops=2 * 6 * toks * 2 * items * q)(table, back)
    rest = swap(part)
    first = lane == 0
    return jnp.concatenate([jnp.where(first, part, rest), jnp.where(first, rest, part)], axis=1)


def solution(mesh):
    return jax.shard_map(
        per_device,
        mesh=mesh,
        in_specs=(
            P(("grp", "ep"), None),
            P(("grp", "ep"), None),
            P(("grp", "ep"), None),
            P(),
            P("ep", None, "tp"),
            P("ep", None, "tp"),
            P("ep", "tp", None),
        ),
        out_specs=P(("grp", "ep"), None),
        check_vma=False,
    )
```

```python
import functools

import jax
import jax.numpy as jnp
from jax import lax
from jax.experimental import pallas as pl
from jax.experimental.pallas import tpu as pltpu
from jax.sharding import PartitionSpec as P

EPS = 1e-06
BF = jnp.bfloat16
F32 = jnp.float32
VMEM = pl.BlockSpec(memory_space=pltpu.VMEM)
SMEM = pl.BlockSpec(memory_space=pltpu.SMEM)
HBM = pl.BlockSpec(memory_space=pltpu.HBM)
LIMIT = 16 * 1024 * 1024
QUARTERS = 4
GROUP = 8


def dot(a, b):
    return jnp.dot(a, b, preferred_element_type=F32)


def iota(shape, dim):
    return lax.broadcasted_iota(jnp.int32, shape, dim)


def div_const(x, n):
    return (x * (-(-(1 << 17) // n))) >> 17


def bf(mask):
    return jnp.where(mask, 1.0, 0.0).astype(BF)


def call(body, outs, in_specs, scratch=(), flops=0):
    return pl.pallas_call(
        body,
        out_shape=outs,
        in_specs=in_specs,
        out_specs=jax.tree.map(lambda _: VMEM, outs),
        scratch_shapes=list(scratch),
        compiler_params=pltpu.CompilerParams(vmem_limit_bytes=LIMIT),
        cost_estimate=pl.CostEstimate(flops=flops, bytes_accessed=0, transcendentals=0),
    )


def prep_body(
    lane_ref, tok_hbm, gain_hbm, rt_hbm, wg_hbm, wu_hbm, wd_hbm,
    out_ref, wg_ref, wu_ref, wd_ref,
    tok_ref, gain_ref, rt_ref, stack_ref, sems, *, experts, slots,
):
    pairs = (
        (tok_hbm, tok_ref), (gain_hbm, gain_ref), (rt_hbm, rt_ref),
        (wg_hbm, wg_ref), (wu_hbm, wu_ref), (wd_hbm, wd_ref),
    )
    copies = [pltpu.make_async_copy(a, b, sems.at[i]) for i, (a, b) in enumerate(pairs)]
    for c in copies:
        c.start()
    for c in copies[:3]:
        c.wait()
    rows, width = tok_ref.shape
    q = width // QUARTERS
    xf = tok_ref[...].astype(F32)
    var = jnp.mean(xf * xf, axis=-1, keepdims=True)
    normed = (xf * lax.rsqrt(var + EPS) * gain_ref[...]).astype(BF)
    for h in range(QUARTERS):
        stack_ref[h * rows : (h + 1) * rows, :] = normed[:, h * q : (h + 1) * q]
    rt = rt_ref[...]
    e_of = iota((experts, rows), 0)
    chosen = jnp.zeros((experts, rows), F32)
    for k in range(rt.shape[0]):
        chosen = chosen + (e_of == rt[k : k + 1, :]).astype(F32)
    upper = bf(iota((rows, rows), 0) < iota((rows, rows), 1))
    rel = dot(chosen.astype(BF), upper) - (lane_ref[0] * slots).astype(F32)
    place = jnp.where((chosen > 0) & (rel >= 0) & (rel < slots), rel, -1.0).astype(BF)
    wide = QUARTERS * rows
    t2 = iota((rows, wide), 1)
    quarter = div_const(t2, rows)
    spread = dot(place, bf(t2 - quarter * rows == iota((rows, wide), 0)))
    quarter = div_const(iota((experts, wide), 1), rows).astype(F32)
    code = jnp.where(spread >= 0, spread + 16.0 * quarter, -1.0).astype(BF)
    message = QUARTERS * slots
    block = GROUP * message
    r = iota((block, wide), 0)
    left = r - div_const(r, message) * message
    part = div_const(left, slots)
    want = (left + part * (16 - slots)).astype(F32)
    e_row = div_const(iota((block, experts), 0), message)
    e_col = iota((block, experts), 1)
    stacked = stack_ref[...]
    for b in range(experts // GROUP):
        one = bf(dot(bf(e_col == e_row + b * GROUP), code) == want)
        out_ref[b * block : (b + 1) * block, :] = dot(one, stacked).astype(BF)
    for c in copies[3:]:
        c.wait()


def sort_matrix(slots, transposed):
    message = QUARTERS * slots
    n = GROUP * message
    each = GROUP * slots
    qdim, pdim = (1, 0) if transposed else (0, 1)
    qq = iota((n, n), qdim)
    h = div_const(qq, each)
    i = qq - h * each
    b = div_const(i, slots)
    src = b * (message - slots) + h * slots + i
    return bf(iota((n, n), pdim) == src)


def unpack(x_ref, rows_ref, slots):
    n = GROUP * QUARTERS * slots
    each = GROUP * slots
    q = x_ref.shape[1]
    perm = sort_matrix(slots, False)
    for b in range(x_ref.shape[0] // n):
        got = dot(perm, x_ref[b * n : (b + 1) * n, :]).astype(BF)
        for h in range(QUARTERS):
            rows_ref[b * each : (b + 1) * each, h * q : (h + 1) * q] = got[h * each : (h + 1) * each, :]


def pack(y, out_ref, slots):
    n = GROUP * QUARTERS * slots
    each = GROUP * slots
    q = out_ref.shape[1]
    perm = sort_matrix(slots, True)
    for b in range(y.shape[0] // each):
        part = y[b * each : (b + 1) * each]
        stacked = jnp.concatenate([part[:, h * q : (h + 1) * q] for h in range(QUARTERS)], axis=0)
        out_ref[b * n : (b + 1) * n, :] = dot(perm, stacked).astype(BF)


def ffn_body(x_ref, wg_ref, wu_ref, wd_ref, out_ref, rows_ref, hid_ref, *, slots):
    unpack(x_ref, rows_ref, slots)
    rows = rows_ref[...]
    for n in range(hid_ref.shape[1] // 128):
        cols = slice(n * 128, (n + 1) * 128)
        both = dot(rows, jnp.concatenate([wg_ref[:, cols], wu_ref[:, cols]], axis=1))
        g, u = both[:, :128], both[:, 128:]
        hid_ref[:, cols] = ((0.5 * g) * (1.0 + jnp.tanh(0.5 * g)) * u).astype(BF)
    y = dot(hid_ref[...], wd_ref[...]).astype(BF)
    pack(y, out_ref, slots)


def table_body(lane_ref, rt_ref, gt_ref, mix_ref, *, slots, experts):
    toks, top = rt_ref.shape
    e_of = iota((toks, experts), 1)
    chosen = jnp.zeros((toks, experts), F32)
    gate = jnp.zeros((toks, experts), F32)
    for k in range(top):
        hit = e_of == rt_ref[:, k : k + 1]
        chosen = chosen + hit.astype(F32)
        gate = gate + jnp.where(hit, gt_ref[:, k : k + 1], 0.0)
    lower = bf(iota((toks, toks), 1) < iota((toks, toks), 0))
    rel = dot(lower, chosen.astype(BF)) - ((1 - lane_ref[0]) * slots).astype(F32)
    place = jnp.where((chosen > 0) & (rel >= 0) & (rel < slots), rel, -1.0).astype(BF)
    g1 = gate.astype(BF)
    rest = gate - g1.astype(F32)
    g2 = rest.astype(BF)
    g3 = (rest - g2.astype(F32)).astype(BF)
    n = slots * experts
    r = iota((1, n), 1)
    e_r = div_const(r, slots)
    slot = (r - e_r * slots).astype(F32)
    rep = bf(iota((experts, n), 0) == e_r)
    here = dot(place, rep) == slot
    for i, piece in enumerate((g1, g2, g3)):
        mix_ref[i * toks : (i + 1) * toks, :] = jnp.where(here, dot(piece, rep), 0.0).astype(BF)


def add_body(a_ref, b_ref, out_ref):
    out_ref[...] = (a_ref[...].astype(F32) + b_ref[...].astype(F32)).astype(BF)


def last_body(mix_ref, back_ref, out_ref, rows_ref, *, slots):
    toks = out_ref.shape[0]
    unpack(back_ref, rows_ref, slots)
    s = dot(mix_ref[...], rows_ref[...])
    out_ref[...] = s[:toks] + s[toks : 2 * toks] + s[2 * toks :]


def per_device(tokens, routes, gates, norm_gain, w_gate, w_up, w_down):
    toks, width = tokens.shape
    top = routes.shape[1]
    experts = lax.axis_size("ep")
    cap = max(2, min(toks, 3 * toks * top // experts))
    slots = -(-cap // 2)
    q = width // QUARTERS
    ff = w_gate.shape[2]
    items = experts * slots
    wide = pltpu.VMEM((QUARTERS * items, q), BF)
    swap = lambda v: lax.ppermute(v, "tp", [(0, 1), (1, 0)])
    lanes = lax.axis_index("tp").astype(jnp.int32).reshape(1)
    wg, wu, wd = w_gate[0], w_up[0], w_down[0]

    outgoing, wg, wu, wd = call(
        functools.partial(prep_body, experts=experts, slots=slots),
        (wide, pltpu.VMEM(wg.shape, BF), pltpu.VMEM(wu.shape, BF), pltpu.VMEM(wd.shape, BF)),
        [SMEM] + [HBM] * 6,
        [
            pltpu.VMEM((toks, width), BF),
            pltpu.VMEM((1, width), F32),
            pltpu.VMEM((top, toks), jnp.int32),
            pltpu.VMEM((QUARTERS * toks, q), BF),
            pltpu.SemaphoreType.DMA((6,)),
        ],
        flops=2 * QUARTERS * items * QUARTERS * toks * q,
    )(lanes, *[pltpu.with_memory_space_constraint(v, pltpu.HBM) for v in (tokens, norm_gain.reshape(1, width), routes.T, wg, wu, wd)])
    exchange = lambda v: lax.all_to_all(
        v.reshape(experts, QUARTERS * slots, q), "ep", split_axis=0, concat_axis=0, tiled=True
    ).reshape(QUARTERS * items, q)
    ffn = call(
        functools.partial(ffn_body, slots=slots), wide, [VMEM] * 4,
        [pltpu.VMEM((items, width), BF), pltpu.VMEM((items, ff), BF)], flops=2 * items * width * 3 * ff,
    )
    mine = exchange(outgoing)
    other = swap(mine)
    got = swap(ffn(mine, wg, wu, wd))
    kept = ffn(other, wg, wu, wd)
    table = call(
        functools.partial(table_body, slots=slots, experts=experts), pltpu.VMEM((3 * toks, items), BF),
        [SMEM, VMEM, VMEM], flops=2 * 4 * toks * experts * items,
    )(lanes, routes, gates)
    back = exchange(call(add_body, wide, [VMEM] * 2, flops=QUARTERS * items * q)(kept, got))
    part = call(
        functools.partial(last_body, slots=slots), pltpu.VMEM((toks, width), F32), [VMEM] * 2,
        [pltpu.VMEM((items, width), BF)], flops=2 * 3 * toks * items * width,
    )(table, back)
    return (part + swap(part)).astype(BF)


def solution(mesh):
    return jax.shard_map(
        per_device,
        mesh=mesh,
        in_specs=(
            P(("grp", "ep"), None),
            P(("grp", "ep"), None),
            P(("grp", "ep"), None),
            P(),
            P("ep", None, "tp"),
            P("ep", None, "tp"),
            P("ep", "tp", None),
        ),
        out_specs=P(("grp", "ep"), None),
        check_vma=False,
    )
```

```python
import functools

import jax
import jax.numpy as jnp
from jax import lax
from jax.experimental import pallas as pl
from jax.experimental.pallas import tpu as pltpu
from jax.sharding import PartitionSpec as P

EPS = 1e-06
BF = jnp.bfloat16
F32 = jnp.float32
VMEM = pl.BlockSpec(memory_space=pltpu.VMEM)
SMEM = pl.BlockSpec(memory_space=pltpu.SMEM)
HBM = pl.BlockSpec(memory_space=pltpu.HBM)
LIMIT = 16 * 1024 * 1024
QUARTERS = 4
GROUP = 8


def dot(a, b):
    return jnp.dot(a, b, preferred_element_type=F32)


def iota(shape, dim):
    return lax.broadcasted_iota(jnp.int32, shape, dim)


def div_const(x, n):
    return (x * (-(-(1 << 17) // n))) >> 17


def bf(mask):
    return jnp.where(mask, 1.0, 0.0).astype(BF)


def call(body, outs, in_specs, scratch=(), flops=0):
    return pl.pallas_call(
        body,
        out_shape=outs,
        in_specs=in_specs,
        out_specs=jax.tree.map(lambda _: VMEM, outs),
        scratch_shapes=list(scratch),
        compiler_params=pltpu.CompilerParams(vmem_limit_bytes=LIMIT),
        cost_estimate=pl.CostEstimate(flops=flops, bytes_accessed=0, transcendentals=0),
    )


def start_all(pairs, sems):
    copies = [pltpu.make_async_copy(a, b, sems.at[i]) for i, (a, b) in enumerate(pairs)]
    for c in copies:
        c.start()
    return copies


def prep_body(
    lane_ref, tok_hbm, gain_hbm, rt_hbm, wg_hbm, wu_hbm,
    out_ref, wg_ref, wu_ref,
    tok_ref, gain_ref, rt_ref, stack_ref, sems, *, experts, slots,
):
    early = wg_ref.shape[1]
    copies = start_all(
        (
            (rt_hbm, rt_ref), (tok_hbm, tok_ref), (gain_hbm, gain_ref),
            (wg_hbm.at[:, :early], wg_ref), (wu_hbm.at[:, :early], wu_ref),
        ),
        sems,
    )
    for c in copies[:3]:
        c.wait()
    rows, width = tok_ref.shape
    q = width // QUARTERS
    xf = tok_ref[...].astype(F32)
    var = jnp.mean(xf * xf, axis=-1, keepdims=True)
    normed = (xf * lax.rsqrt(var + EPS) * gain_ref[...]).astype(BF)
    for h in range(QUARTERS):
        stack_ref[h * rows : (h + 1) * rows, :] = normed[:, h * q : (h + 1) * q]
    rt = rt_ref[...]
    e_of = iota((experts, rows), 0)
    chosen = jnp.zeros((experts, rows), F32)
    for k in range(rt.shape[0]):
        chosen = chosen + (e_of == rt[k : k + 1, :]).astype(F32)
    upper = bf(iota((rows, rows), 0) < iota((rows, rows), 1))
    rel = dot(chosen.astype(BF), upper) - (lane_ref[0] * slots).astype(F32)
    place = jnp.where((chosen > 0) & (rel >= 0) & (rel < slots), rel, -1.0).astype(BF)
    wide = QUARTERS * rows
    t2 = iota((rows, wide), 1)
    quarter = div_const(t2, rows)
    spread = dot(place, bf(t2 - quarter * rows == iota((rows, wide), 0)))
    quarter = div_const(iota((experts, wide), 1), rows).astype(F32)
    code = jnp.where(spread >= 0, spread + 16.0 * quarter, -1.0).astype(BF)
    message = QUARTERS * slots
    block = GROUP * message
    r = iota((block, wide), 0)
    left = r - div_const(r, message) * message
    part = div_const(left, slots)
    want = (left + part * (16 - slots)).astype(F32)
    e_row = div_const(iota((block, experts), 0), message)
    e_col = iota((block, experts), 1)
    stacked = stack_ref[...]
    for b in range(experts // GROUP):
        one = bf(dot(bf(e_col == e_row + b * GROUP), code) == want)
        out_ref[b * block : (b + 1) * block, :] = dot(one, stacked).astype(BF)
    for c in copies[3:]:
        c.wait()


def sort_matrix(slots, transposed):
    message = QUARTERS * slots
    n = GROUP * message
    each = GROUP * slots
    qdim, pdim = (1, 0) if transposed else (0, 1)
    qq = iota((n, n), qdim)
    h = div_const(qq, each)
    i = qq - h * each
    b = div_const(i, slots)
    src = b * (message - slots) + h * slots + i
    return bf(iota((n, n), pdim) == src)


def unpack(x_ref, rows_ref, slots):
    n = GROUP * QUARTERS * slots
    each = GROUP * slots
    q = x_ref.shape[1]
    perm = sort_matrix(slots, False)
    for b in range(x_ref.shape[0] // n):
        got = dot(perm, x_ref[b * n : (b + 1) * n, :]).astype(BF)
        for h in range(QUARTERS):
            rows_ref[b * each : (b + 1) * each, h * q : (h + 1) * q] = got[h * each : (h + 1) * each, :]


def pack(y, out_ref, slots):
    n = GROUP * QUARTERS * slots
    each = GROUP * slots
    q = out_ref.shape[1]
    perm = sort_matrix(slots, True)
    for b in range(y.shape[0] // each):
        part = y[b * each : (b + 1) * each]
        stacked = jnp.concatenate([part[:, h * q : (h + 1) * q] for h in range(QUARTERS)], axis=0)
        out_ref[b * n : (b + 1) * n, :] = dot(perm, stacked).astype(BF)


def columns(first_ref, second_ref, n):
    at = n * 128
    ref, at = (first_ref, at) if at < first_ref.shape[1] else (second_ref, at - first_ref.shape[1])
    return ref[:, at : at + 128]


def hidden_units(rows, wg1_ref, wu1_ref, wg2_ref, wu2_ref, hid_ref, ready):
    for n in range(hid_ref.shape[1] // 128):
        ready(n)
        w = jnp.concatenate([columns(wg1_ref, wg2_ref, n), columns(wu1_ref, wu2_ref, n)], axis=1)
        both = dot(rows, w)
        g, u = both[:, :128], both[:, 128:]
        hid_ref[:, n * 128 : (n + 1) * 128] = ((0.5 * g) * (1.0 + jnp.tanh(0.5 * g)) * u).astype(BF)


def own_body(
    lane_ref, x_ref, wg1_ref, wu1_ref, wg_hbm, wu_hbm, wd_hbm, rt_hbm, gt_hbm,
    out_ref, wg2_ref, wu2_ref, wd_ref, mix_ref,
    rows_ref, hid_ref, rt_ref, gt_ref, sems, *, slots, experts,
):
    early, late = wg1_ref.shape[1], wg2_ref.shape[1]
    pairs = []
    for at in range(0, late, 128):
        for hbm, ref in ((wg_hbm, wg2_ref), (wu_hbm, wu2_ref)):
            pairs.append((hbm.at[:, early + at : early + at + 128], ref.at[:, at : at + 128]))
    pairs += [(wd_hbm, wd_ref), (rt_hbm, rt_ref), (gt_hbm, gt_ref)]
    copies = start_all(pairs, sems)

    def ready(n):
        k = n - early // 128
        if k >= 0:
            copies[2 * k].wait()
            copies[2 * k + 1].wait()

    unpack(x_ref, rows_ref, slots)
    hidden_units(rows_ref[...], wg1_ref, wu1_ref, wg2_ref, wu2_ref, hid_ref, ready)
    for c in copies[-3:]:
        c.wait()
    out_ref[...] = dot(hid_ref[...], wd_ref[...]).astype(BF)
    table(lane_ref, rt_ref[...], gt_ref[...], mix_ref, slots, experts)


def other_body(x_ref, wg1_ref, wu1_ref, wg2_ref, wu2_ref, wd_ref, out_ref, rows_ref, hid_ref, *, slots):
    unpack(x_ref, rows_ref, slots)
    hidden_units(rows_ref[...], wg1_ref, wu1_ref, wg2_ref, wu2_ref, hid_ref, lambda n: None)
    out_ref[...] = dot(hid_ref[...], wd_ref[...]).astype(BF)


def table(lane_ref, rt, gt, mix_ref, slots, experts):
    top, toks = rt.shape
    e_of = iota((experts, toks), 0)
    chosen = jnp.zeros((experts, toks), F32)
    gate = jnp.zeros((experts, toks), F32)
    for k in range(top):
        hit = e_of == rt[k : k + 1, :]
        chosen = chosen + hit.astype(F32)
        gate = gate + jnp.where(hit, gt[k : k + 1, :], 0.0)
    upper = bf(iota((toks, toks), 0) < iota((toks, toks), 1))
    rel = dot(chosen.astype(BF), upper) - ((1 - lane_ref[0]) * slots).astype(F32)
    place = jnp.where((chosen > 0) & (rel >= 0) & (rel < slots), rel, -1.0).T.astype(BF)
    gate = gate.T
    g1 = gate.astype(BF)
    rest = gate - g1.astype(F32)
    g2 = rest.astype(BF)
    g3 = (rest - g2.astype(F32)).astype(BF)
    n = slots * experts
    r = iota((1, n), 1)
    e_r = div_const(r, slots)
    slot = (r - e_r * slots).astype(F32)
    rep = bf(iota((experts, n), 0) == e_r)
    here = dot(place, rep) == slot
    for i, piece in enumerate((g1, g2, g3)):
        mix_ref[i * toks : (i + 1) * toks, :] = jnp.where(here, dot(piece, rep), 0.0).astype(BF)


def add_body(a_ref, b_ref, out_ref, *, slots):
    pack((a_ref[...].astype(F32) + b_ref[...].astype(F32)).astype(BF), out_ref, slots)


def last_body(mix_ref, back_ref, out_ref, rows_ref, *, slots):
    toks = out_ref.shape[0]
    unpack(back_ref, rows_ref, slots)
    s = dot(mix_ref[...], rows_ref[...])
    out_ref[...] = s[:toks] + s[toks : 2 * toks] + s[2 * toks :]


def per_device(tokens, routes, gates, norm_gain, w_gate, w_up, w_down):
    toks, width = tokens.shape
    top = routes.shape[1]
    experts = lax.axis_size("ep")
    cap = max(2, min(toks, 3 * toks * top // experts))
    slots = -(-cap // 2)
    q = width // QUARTERS
    ff = w_gate.shape[2]
    items = experts * slots
    wide = pltpu.VMEM((QUARTERS * items, q), BF)
    tall = pltpu.VMEM((items, width), BF)
    early = ff // 128 * 3 // 7 * 128
    late = ff - early
    swap = lambda v: lax.ppermute(v, "tp", [(0, 1), (1, 0)])
    lanes = lax.axis_index("tp").astype(jnp.int32).reshape(1)
    in_hbm = lambda *vs: [pltpu.with_memory_space_constraint(v, pltpu.HBM) for v in vs]
    wg, wu, wd = w_gate[0], w_up[0], w_down[0]
    rt = routes.T

    outgoing, wg1, wu1 = call(
        functools.partial(prep_body, experts=experts, slots=slots),
        (wide, pltpu.VMEM((width, early), BF), pltpu.VMEM((width, early), BF)),
        [SMEM] + [HBM] * 5,
        [
            pltpu.VMEM((toks, width), BF),
            pltpu.VMEM((1, width), F32),
            pltpu.VMEM((top, toks), jnp.int32),
            pltpu.VMEM((QUARTERS * toks, q), BF),
            pltpu.SemaphoreType.DMA((5,)),
        ],
        flops=2 * QUARTERS * items * QUARTERS * toks * q,
    )(lanes, *in_hbm(tokens, norm_gain.reshape(1, width), rt, wg, wu))
    exchange = lambda v: lax.all_to_all(
        v.reshape(experts, QUARTERS * slots, q), "ep", split_axis=0, concat_axis=0, tiled=True
    ).reshape(QUARTERS * items, q)
    mine = exchange(outgoing)
    other = swap(mine)
    work = 2 * items * width * 3 * ff
    held = [pltpu.VMEM((items, width), BF), pltpu.VMEM((items, ff), BF)]
    sent, wg2, wu2, wd1, mix = call(
        functools.partial(own_body, slots=slots, experts=experts),
        (
            tall, pltpu.VMEM((width, late), BF), pltpu.VMEM((width, late), BF),
            pltpu.VMEM(wd.shape, BF), pltpu.VMEM((3 * toks, items), BF),
        ),
        [SMEM] + [VMEM] * 3 + [HBM] * 5,
        [
            *held,
            pltpu.VMEM((top, toks), jnp.int32),
            pltpu.VMEM((top, toks), F32),
            pltpu.SemaphoreType.DMA((late // 128 * 2 + 3,)),
        ],
        flops=work,
    )(lanes, mine, wg1, wu1, *in_hbm(wg, wu, wd, rt, gates.T))
    got = swap(sent)
    kept = call(functools.partial(other_body, slots=slots), tall, [VMEM] * 6, held, flops=work)(
        other, wg1, wu1, wg2, wu2, wd1
    )
    summed = call(functools.partial(add_body, slots=slots), wide, [VMEM] * 2, flops=items * width)(kept, got)
    back = exchange(summed)
    part = call(
        functools.partial(last_body, slots=slots), pltpu.VMEM((toks, width), F32), [VMEM] * 2,
        [pltpu.VMEM((items, width), BF)], flops=2 * 3 * toks * items * width,
    )(mix, back)
    return (part + swap(part)).astype(BF)


def solution(mesh):
    return jax.shard_map(
        per_device,
        mesh=mesh,
        in_specs=(
            P(("grp", "ep"), None),
            P(("grp", "ep"), None),
            P(("grp", "ep"), None),
            P(),
            P("ep", None, "tp"),
            P("ep", None, "tp"),
            P("ep", "tp", None),
        ),
        out_specs=P(("grp", "ep"), None),
        check_vma=False,
    )
```

```python
import functools

import jax
import jax.numpy as jnp
from jax import lax
from jax.experimental import pallas as pl
from jax.experimental.pallas import tpu as pltpu
from jax.sharding import PartitionSpec as P

EPS = 1e-06
BF = jnp.bfloat16
F32 = jnp.float32
VMEM = pl.BlockSpec(memory_space=pltpu.VMEM)
SMEM = pl.BlockSpec(memory_space=pltpu.SMEM)
HBM = pl.BlockSpec(memory_space=pltpu.HBM)
LIMIT = 16 * 1024 * 1024
QUARTERS = 4
GROUP = 8


def dot(a, b):
    return jnp.dot(a, b, preferred_element_type=F32)


def iota(shape, dim):
    return lax.broadcasted_iota(jnp.int32, shape, dim)


def div_const(x, n):
    return (x * (-(-(1 << 17) // n))) >> 17


def bf(mask):
    return jnp.where(mask, 1.0, 0.0).astype(BF)


def call(body, outs, in_specs, scratch=(), flops=0):
    return pl.pallas_call(
        body,
        out_shape=outs,
        in_specs=in_specs,
        out_specs=jax.tree.map(lambda _: VMEM, outs),
        scratch_shapes=list(scratch),
        compiler_params=pltpu.CompilerParams(vmem_limit_bytes=LIMIT),
        cost_estimate=pl.CostEstimate(flops=flops, bytes_accessed=0, transcendentals=0),
    )


def start_all(pairs, sems):
    copies = [pltpu.make_async_copy(a, b, sems.at[i]) for i, (a, b) in enumerate(pairs)]
    for c in copies:
        c.start()
    return copies


def prep_body(
    lane_ref, tok_hbm, gain_hbm, rt_hbm, wg_hbm, wu_hbm,
    out_ref, wg_ref, wu_ref,
    tok_ref, gain_ref, rt_ref, stack_ref, sems, *, experts, slots,
):
    early = wg_ref.shape[1]
    copies = start_all(
        (
            (rt_hbm, rt_ref), (tok_hbm, tok_ref), (gain_hbm, gain_ref),
            (wg_hbm.at[:, :early], wg_ref), (wu_hbm.at[:, :early], wu_ref),
        ),
        sems,
    )
    for c in copies[:3]:
        c.wait()
    rows, width = tok_ref.shape
    q = width // QUARTERS
    xf = tok_ref[...].astype(F32)
    var = jnp.mean(xf * xf, axis=-1, keepdims=True)
    normed = (xf * lax.rsqrt(var + EPS) * gain_ref[...]).astype(BF)
    for h in range(QUARTERS):
        stack_ref[h * rows : (h + 1) * rows, :] = normed[:, h * q : (h + 1) * q]
    wide = QUARTERS * rows
    rt = jnp.concatenate([rt_ref[...]] * QUARTERS, axis=1)
    e_of = iota((experts, wide), 0)
    chosen = jnp.zeros((experts, wide), F32)
    for k in range(rt.shape[0]):
        chosen = chosen + (e_of == rt[k : k + 1, :]).astype(F32)
    t2 = iota((rows, wide), 1)
    upper = bf(iota((rows, wide), 0) < t2 - div_const(t2, rows) * rows)
    rel = dot(chosen[:, :rows].astype(BF), upper) - (lane_ref[0] * slots).astype(F32)
    quarter = div_const(iota((experts, wide), 1), rows).astype(F32)
    code = jnp.where((chosen > 0) & (rel >= 0) & (rel < slots), rel + 16.0 * quarter, -1.0).astype(BF)
    message = QUARTERS * slots
    block = GROUP * message
    r = iota((block, wide), 0)
    left = r - div_const(r, message) * message
    part = div_const(left, slots)
    want = (left + part * (16 - slots)).astype(F32)
    e_row = div_const(iota((block, experts), 0), message)
    e_col = iota((block, experts), 1)
    stacked = stack_ref[...]
    for b in range(experts // GROUP):
        one = bf(dot(bf(e_col == e_row + b * GROUP), code) == want)
        out_ref[b * block : (b + 1) * block, :] = dot(one, stacked).astype(BF)
    for c in copies[3:]:
        c.wait()


def sort_matrix(slots, transposed):
    message = QUARTERS * slots
    n = GROUP * message
    each = GROUP * slots
    qdim, pdim = (1, 0) if transposed else (0, 1)
    qq = iota((n, n), qdim)
    h = div_const(qq, each)
    i = qq - h * each
    b = div_const(i, slots)
    src = b * (message - slots) + h * slots + i
    return bf(iota((n, n), pdim) == src)


def unpack(x_ref, rows_ref, slots):
    n = GROUP * QUARTERS * slots
    each = GROUP * slots
    q = x_ref.shape[1]
    perm = sort_matrix(slots, False)
    for b in range(x_ref.shape[0] // n):
        got = dot(perm, x_ref[b * n : (b + 1) * n, :]).astype(BF)
        for h in range(QUARTERS):
            rows_ref[b * each : (b + 1) * each, h * q : (h + 1) * q] = got[h * each : (h + 1) * each, :]


def pack(y, out_ref, slots):
    n = GROUP * QUARTERS * slots
    each = GROUP * slots
    q = out_ref.shape[1]
    perm = sort_matrix(slots, True)
    for b in range(y.shape[0] // each):
        part = y[b * each : (b + 1) * each]
        stacked = jnp.concatenate([part[:, h * q : (h + 1) * q] for h in range(QUARTERS)], axis=0)
        out_ref[b * n : (b + 1) * n, :] = dot(perm, stacked).astype(BF)


def columns(first_ref, second_ref, n):
    at = n * 128
    ref, at = (first_ref, at) if at < first_ref.shape[1] else (second_ref, at - first_ref.shape[1])
    return ref[:, at : at + 128]


def hidden_units(rows, wg1_ref, wu1_ref, wg2_ref, wu2_ref, hid_ref, ready):
    for n in range(hid_ref.shape[1] // 128):
        ready(n)
        w = jnp.concatenate([columns(wg1_ref, wg2_ref, n), columns(wu1_ref, wu2_ref, n)], axis=1)
        both = dot(rows, w)
        g, u = both[:, :128], both[:, 128:]
        hid_ref[:, n * 128 : (n + 1) * 128] = ((0.5 * g) * (1.0 + jnp.tanh(0.5 * g)) * u).astype(BF)


def own_body(
    x_ref, wg1_ref, wu1_ref, wg_hbm, wu_hbm, wd_hbm,
    out_ref, wg2_ref, wu2_ref, wd_ref, rows_ref, hid_ref, sems, *, slots,
):
    early = wg1_ref.shape[1]
    copies = start_all(
        ((wg_hbm.at[:, early:], wg2_ref), (wu_hbm.at[:, early:], wu2_ref), (wd_hbm, wd_ref)), sems
    )

    def ready(n):
        if n * 128 == early:
            copies[0].wait()
            copies[1].wait()

    unpack(x_ref, rows_ref, slots)
    hidden_units(rows_ref[...], wg1_ref, wu1_ref, wg2_ref, wu2_ref, hid_ref, ready)
    copies[2].wait()
    out_ref[...] = dot(hid_ref[...], wd_ref[...]).astype(BF)


def other_body(
    lane_ref, x_ref, wg1_ref, wu1_ref, wg2_ref, wu2_ref, wd_ref, rt_ref, gt_ref,
    out_ref, mix_ref, rows_ref, hid_ref, *, slots, experts,
):
    unpack(x_ref, rows_ref, slots)
    table(lane_ref, rt_ref[...], gt_ref[...], mix_ref, slots, experts)
    hidden_units(rows_ref[...], wg1_ref, wu1_ref, wg2_ref, wu2_ref, hid_ref, lambda n: None)
    out_ref[...] = dot(hid_ref[...], wd_ref[...]).astype(BF)


def table(lane_ref, rt, gt, mix_ref, slots, experts):
    top, toks = rt.shape
    e_of = iota((experts, toks), 0)
    chosen = jnp.zeros((experts, toks), F32)
    gate = jnp.zeros((experts, toks), F32)
    for k in range(top):
        hit = e_of == rt[k : k + 1, :]
        chosen = chosen + hit.astype(F32)
        gate = gate + jnp.where(hit, gt[k : k + 1, :], 0.0)
    upper = bf(iota((toks, toks), 0) < iota((toks, toks), 1))
    rel = dot(chosen.astype(BF), upper) - ((1 - lane_ref[0]) * slots).astype(F32)
    place = jnp.where((chosen > 0) & (rel >= 0) & (rel < slots), rel, -1.0).T.astype(BF)
    gate = gate.T
    g1 = gate.astype(BF)
    rest = gate - g1.astype(F32)
    g2 = rest.astype(BF)
    g3 = (rest - g2.astype(F32)).astype(BF)
    n = slots * experts
    r = iota((1, n), 1)
    e_r = div_const(r, slots)
    slot = (r - e_r * slots).astype(F32)
    rep = bf(iota((experts, n), 0) == e_r)
    here = dot(place, rep) == slot
    for i, piece in enumerate((g1, g2, g3)):
        mix_ref[i * toks : (i + 1) * toks, :] = jnp.where(here, dot(piece, rep), 0.0).astype(BF)


def add_body(a_ref, b_ref, out_ref, *, slots):
    pack((a_ref[...].astype(F32) + b_ref[...].astype(F32)).astype(BF), out_ref, slots)


def last_body(mix_ref, back_ref, out_ref, rows_ref, *, slots):
    toks = out_ref.shape[0]
    unpack(back_ref, rows_ref, slots)
    s = dot(mix_ref[...], rows_ref[...])
    out_ref[...] = s[:toks] + s[toks : 2 * toks] + s[2 * toks :]


def per_device(tokens, routes, gates, norm_gain, w_gate, w_up, w_down):
    toks, width = tokens.shape
    top = routes.shape[1]
    experts = lax.axis_size("ep")
    cap = max(2, min(toks, 3 * toks * top // experts))
    slots = -(-cap // 2)
    q = width // QUARTERS
    ff = w_gate.shape[2]
    items = experts * slots
    wide = pltpu.VMEM((QUARTERS * items, q), BF)
    tall = pltpu.VMEM((items, width), BF)
    early = ff // 128 * 5 // 7 * 128
    late = ff - early
    swap = lambda v: lax.ppermute(v, "tp", [(0, 1), (1, 0)])
    lanes = lax.axis_index("tp").astype(jnp.int32).reshape(1)
    in_hbm = lambda *vs: [pltpu.with_memory_space_constraint(v, pltpu.HBM) for v in vs]
    wg, wu, wd = w_gate[0], w_up[0], w_down[0]
    rt = routes.T

    outgoing, wg1, wu1 = call(
        functools.partial(prep_body, experts=experts, slots=slots),
        (wide, pltpu.VMEM((width, early), BF), pltpu.VMEM((width, early), BF)),
        [SMEM] + [HBM] * 5,
        [
            pltpu.VMEM((toks, width), BF),
            pltpu.VMEM((1, width), F32),
            pltpu.VMEM((top, toks), jnp.int32),
            pltpu.VMEM((QUARTERS * toks, q), BF),
            pltpu.SemaphoreType.DMA((5,)),
        ],
        flops=2 * QUARTERS * items * QUARTERS * toks * q,
    )(lanes, *in_hbm(tokens, norm_gain.reshape(1, width), rt, wg, wu))
    exchange = lambda v: lax.all_to_all(
        v.reshape(experts, QUARTERS * slots, q), "ep", split_axis=0, concat_axis=0, tiled=True
    ).reshape(QUARTERS * items, q)
    mine = exchange(outgoing)
    other = swap(mine)
    work = 2 * items * width * 3 * ff
    held = [pltpu.VMEM((items, width), BF), pltpu.VMEM((items, ff), BF)]
    sent, wg2, wu2, wd1 = call(
        functools.partial(own_body, slots=slots),
        (tall, pltpu.VMEM((width, late), BF), pltpu.VMEM((width, late), BF), pltpu.VMEM(wd.shape, BF)),
        [VMEM] * 3 + [HBM] * 3, [*held, pltpu.SemaphoreType.DMA((3,))], flops=work,
    )(mine, wg1, wu1, *in_hbm(wg, wu, wd))
    got = swap(sent)
    kept, mix = call(
        functools.partial(other_body, slots=slots, experts=experts),
        (tall, pltpu.VMEM((3 * toks, items), BF)), [SMEM] + [VMEM] * 8, held, flops=work,
    )(lanes, other, wg1, wu1, wg2, wu2, wd1, rt, gates.T)
    summed = call(functools.partial(add_body, slots=slots), wide, [VMEM] * 2, flops=items * width)(kept, got)
    back = exchange(summed)
    part = call(
        functools.partial(last_body, slots=slots), pltpu.VMEM((toks, width), F32), [VMEM] * 2,
        [pltpu.VMEM((items, width), BF)], flops=2 * 3 * toks * items * width,
    )(mix, back)
    return (part + swap(part)).astype(BF)


def solution(mesh):
    return jax.shard_map(
        per_device,
        mesh=mesh,
        in_specs=(
            P(("grp", "ep"), None),
            P(("grp", "ep"), None),
            P(("grp", "ep"), None),
            P(),
            P("ep", None, "tp"),
            P("ep", None, "tp"),
            P("ep", "tp", None),
        ),
        out_specs=P(("grp", "ep"), None),
        check_vma=False,
    )
```

```python
import functools

import jax
import jax.numpy as jnp
from jax import lax
from jax.experimental import pallas as pl
from jax.experimental.pallas import tpu as pltpu
from jax.sharding import PartitionSpec as P

EPS = 1e-06
BF = jnp.bfloat16
F32 = jnp.float32
VMEM = pl.BlockSpec(memory_space=pltpu.VMEM)
SMEM = pl.BlockSpec(memory_space=pltpu.SMEM)
HBM = pl.BlockSpec(memory_space=pltpu.HBM)
LIMIT = 16 * 1024 * 1024


def dot(a, b):
    return jnp.dot(a, b, preferred_element_type=F32)


def iota(shape, dim):
    return lax.broadcasted_iota(jnp.int32, shape, dim)


def div_const(x, n):
    return (x * (-(-(1 << 17) // n))) >> 17


def bf(mask):
    return jnp.where(mask, 1.0, 0.0).astype(BF)


def flat(ref):
    pairs, two, width = ref.shape
    return ref[...].reshape(pairs * two, width)


def call(body, outs, in_specs, scratch=(), flops=0):
    return pl.pallas_call(
        body,
        out_shape=outs,
        in_specs=in_specs,
        out_specs=jax.tree.map(lambda _: VMEM, outs),
        scratch_shapes=list(scratch),
        compiler_params=pltpu.CompilerParams(vmem_limit_bytes=LIMIT),
        cost_estimate=pl.CostEstimate(flops=flops, bytes_accessed=0, transcendentals=0),
    )


def start_all(pairs, sems):
    copies = [pltpu.make_async_copy(a, b, sems.at[i]) for i, (a, b) in enumerate(pairs)]
    for c in copies:
        c.start()
    return copies


def slot_of(chosen, core, slots):
    toks = chosen.shape[1]
    upper = bf(iota((toks, toks), 0) < iota((toks, toks), 1))
    rel = dot(chosen.astype(BF), upper) - (core * slots).astype(F32)
    return jnp.where((chosen > 0) & (rel >= 0) & (rel < slots), rel, -1.0)


def prep_body(
    lane_ref, tok_hbm, gain_hbm, rt_hbm, wg_hbm, wu_hbm,
    out_ref, wg_ref, wu_ref,
    tok_ref, gain_ref, rt_ref, sems, *, experts, slots,
):
    early = wg_ref.shape[1]
    copies = start_all(
        (
            (rt_hbm, rt_ref), (tok_hbm, tok_ref), (gain_hbm, gain_ref),
            (wg_hbm.at[:, :early], wg_ref), (wu_hbm.at[:, :early], wu_ref),
        ),
        sems,
    )
    for c in copies[:3]:
        c.wait()
    toks = tok_ref.shape[0]
    xf = tok_ref[...].astype(F32)
    var = jnp.mean(xf * xf, axis=-1, keepdims=True)
    normed = (xf * lax.rsqrt(var + EPS) * gain_ref[...]).astype(BF)
    e_of = iota((experts, toks), 0)
    chosen = jnp.zeros((experts, toks), F32)
    for k in range(rt_ref.shape[0]):
        chosen = chosen + (e_of == rt_ref[k : k + 1, :]).astype(F32)
    place = slot_of(chosen, lane_ref[0], slots).astype(BF)
    n = slots * experts
    e_row = div_const(iota((n, experts), 0), slots)
    r = iota((n, toks), 0)
    slot = (r - div_const(r, slots) * slots).astype(F32)
    one = bf(dot(bf(iota((n, experts), 1) == e_row), place) == slot)
    out_ref[...] = dot(one, normed).astype(BF).reshape(out_ref.shape)
    for c in copies[3:]:
        c.wait()


def columns(first_ref, second_ref, n):
    at = n * 128
    ref, at = (first_ref, at) if at < first_ref.shape[1] else (second_ref, at - first_ref.shape[1])
    return ref[:, at : at + 128]


def hidden_units(rows, wg1_ref, wu1_ref, wg2_ref, wu2_ref, hid_ref, ready):
    for n in range(hid_ref.shape[1] // 128):
        ready(n)
        w = jnp.concatenate([columns(wg1_ref, wg2_ref, n), columns(wu1_ref, wu2_ref, n)], axis=1)
        both = dot(rows, w)
        g, u = both[:, :128], both[:, 128:]
        hid_ref[:, n * 128 : (n + 1) * 128] = ((0.5 * g) * (1.0 + jnp.tanh(0.5 * g)) * u).astype(BF)


def own_body(
    x_ref, wg1_ref, wu1_ref, wg_hbm, wu_hbm, wd_hbm, out_ref, wg2_ref, wu2_ref, wd_ref, hid_ref, sems
):
    early = wg1_ref.shape[1]
    copies = start_all(
        ((wg_hbm.at[:, early:], wg2_ref), (wu_hbm.at[:, early:], wu2_ref), (wd_hbm, wd_ref)), sems
    )

    def ready(n):
        if n * 128 == early:
            copies[0].wait()
            copies[1].wait()

    hidden_units(flat(x_ref), wg1_ref, wu1_ref, wg2_ref, wu2_ref, hid_ref, ready)
    copies[2].wait()
    out_ref[...] = dot(hid_ref[...], wd_ref[...]).astype(BF)


def other_body(
    lane_ref, x_ref, wg1_ref, wu1_ref, wg2_ref, wu2_ref, wd_ref, rt_ref, gt_ref,
    out_ref, mix_ref, hid_ref, *, slots, experts,
):
    table(lane_ref, rt_ref[...], gt_ref[...], mix_ref, slots, experts)
    hidden_units(flat(x_ref), wg1_ref, wu1_ref, wg2_ref, wu2_ref, hid_ref, lambda n: None)
    out_ref[...] = dot(hid_ref[...], wd_ref[...]).astype(BF)


def table(lane_ref, rt, gt, mix_ref, slots, experts):
    top, toks = rt.shape
    e_of = iota((experts, toks), 0)
    chosen = jnp.zeros((experts, toks), F32)
    gate = jnp.zeros((experts, toks), F32)
    for k in range(top):
        hit = e_of == rt[k : k + 1, :]
        chosen = chosen + hit.astype(F32)
        gate = gate + jnp.where(hit, gt[k : k + 1, :], 0.0)
    place = slot_of(chosen, 1 - lane_ref[0], slots).T.astype(BF)
    gate = gate.T
    g1 = gate.astype(BF)
    rest = gate - g1.astype(F32)
    g2 = rest.astype(BF)
    g3 = (rest - g2.astype(F32)).astype(BF)
    n = slots * experts
    r = iota((1, n), 1)
    e_r = div_const(r, slots)
    slot = (r - e_r * slots).astype(F32)
    rep = bf(iota((experts, n), 0) == e_r)
    here = dot(place, rep) == slot
    for i, piece in enumerate((g1, g2, g3)):
        mix_ref[i * toks : (i + 1) * toks, :] = jnp.where(here, dot(piece, rep), 0.0).astype(BF)


def add_body(a_ref, b_ref, out_ref):
    total = a_ref[...].astype(F32) + b_ref[...].astype(F32)
    out_ref[...] = total.astype(BF).reshape(out_ref.shape)


def last_body(mix_ref, back_ref, out_ref):
    toks = out_ref.shape[0]
    s = dot(mix_ref[...], flat(back_ref))
    out_ref[...] = s[:toks] + s[toks : 2 * toks] + s[2 * toks :]


def per_device(tokens, routes, gates, norm_gain, w_gate, w_up, w_down):
    toks, width = tokens.shape
    top = routes.shape[1]
    experts = lax.axis_size("ep")
    cap = max(2, min(toks, 3 * toks * top // experts))
    slots = -(-cap // 4) * 2
    ff = w_gate.shape[2]
    items = experts * slots
    pairs = pltpu.VMEM((items // 2, 2, width), BF)
    tall = pltpu.VMEM((items, width), BF)
    early = ff // 128 * 5 // 7 * 128
    late = ff - early
    swap = lambda v: lax.ppermute(v, "tp", [(0, 1), (1, 0)])
    lanes = lax.axis_index("tp").astype(jnp.int32).reshape(1)
    in_hbm = lambda *vs: [pltpu.with_memory_space_constraint(v, pltpu.HBM) for v in vs]
    wg, wu, wd = w_gate[0], w_up[0], w_down[0]
    rt = routes.T

    outgoing, wg1, wu1 = call(
        functools.partial(prep_body, experts=experts, slots=slots),
        (pairs, pltpu.VMEM((width, early), BF), pltpu.VMEM((width, early), BF)),
        [SMEM] + [HBM] * 5,
        [
            pltpu.VMEM((toks, width), BF),
            pltpu.VMEM((1, width), F32),
            pltpu.VMEM((top, toks), jnp.int32),
            pltpu.SemaphoreType.DMA((5,)),
        ],
        flops=2 * items * toks * width,
    )(lanes, *in_hbm(tokens, norm_gain.reshape(1, width), rt, wg, wu))
    exchange = lambda v: lax.all_to_all(
        v.reshape(experts, slots // 2, 2, width), "ep", split_axis=0, concat_axis=0, tiled=True
    ).reshape(v.shape)
    mine = exchange(outgoing)
    other = swap(mine)
    work = 2 * items * width * 3 * ff
    held = pltpu.VMEM((items, ff), BF)
    sent, wg2, wu2, wd1 = call(
        own_body,
        (tall, pltpu.VMEM((width, late), BF), pltpu.VMEM((width, late), BF), pltpu.VMEM(wd.shape, BF)),
        [VMEM] * 3 + [HBM] * 3, [held, pltpu.SemaphoreType.DMA((3,))], flops=work,
    )(mine, wg1, wu1, *in_hbm(wg, wu, wd))
    got = swap(sent)
    kept, mix = call(
        functools.partial(other_body, slots=slots, experts=experts),
        (tall, pltpu.VMEM((3 * toks, items), BF)), [SMEM] + [VMEM] * 8, [held], flops=work,
    )(lanes, other, wg1, wu1, wg2, wu2, wd1, rt, gates.T)
    back = exchange(call(add_body, pairs, [VMEM] * 2, flops=items * width)(kept, got))
    part = call(
        last_body, pltpu.VMEM((toks, width), F32), [VMEM] * 2, flops=2 * 3 * toks * items * width
    )(mix, back)
    return (part + swap(part)).astype(BF)


def solution(mesh):
    return jax.shard_map(
        per_device,
        mesh=mesh,
        in_specs=(
            P(("grp", "ep"), None),
            P(("grp", "ep"), None),
            P(("grp", "ep"), None),
            P(),
            P("ep", None, "tp"),
            P("ep", None, "tp"),
            P("ep", "tp", None),
        ),
        out_specs=P(("grp", "ep"), None),
        check_vma=False,
    )
```

```python
import functools

import jax
import jax.numpy as jnp
from jax import lax
from jax.experimental import pallas as pl
from jax.experimental.pallas import tpu as pltpu
from jax.sharding import PartitionSpec as P

EPS = 1e-06
BF = jnp.bfloat16
F32 = jnp.float32
VMEM = pl.BlockSpec(memory_space=pltpu.VMEM)
SMEM = pl.BlockSpec(memory_space=pltpu.SMEM)
HBM = pl.BlockSpec(memory_space=pltpu.HBM)
LIMIT = 16 * 1024 * 1024


def dot(a, b):
    return jnp.dot(a, b, preferred_element_type=F32)


def iota(shape, dim):
    return lax.broadcasted_iota(jnp.int32, shape, dim)


def div_const(x, n):
    return (x * (-(-(1 << 17) // n))) >> 17


def bf(mask):
    return jnp.where(mask, 1.0, 0.0).astype(BF)


def flat(ref):
    pairs, two, width = ref.shape
    return ref[...].reshape(pairs * two, width)


def call(body, outs, in_specs, scratch=(), flops=0):
    return pl.pallas_call(
        body,
        out_shape=outs,
        in_specs=in_specs,
        out_specs=jax.tree.map(lambda _: VMEM, outs),
        scratch_shapes=list(scratch),
        compiler_params=pltpu.CompilerParams(vmem_limit_bytes=LIMIT),
        cost_estimate=pl.CostEstimate(flops=flops, bytes_accessed=0, transcendentals=0),
    )


def start_all(pairs, sems):
    copies = [pltpu.make_async_copy(a, b, sems.at[i]) for i, (a, b) in enumerate(pairs)]
    for c in copies:
        c.start()
    return copies


def slot_of(chosen, core, slots):
    toks = chosen.shape[1]
    upper = bf(iota((toks, toks), 0) < iota((toks, toks), 1))
    rel = dot(chosen.astype(BF), upper) - (core * slots).astype(F32)
    return jnp.where((chosen > 0) & (rel >= 0) & (rel < slots), rel, -1.0)


def prep_body(
    lane_ref, tok_hbm, gain_hbm, rt_hbm, wu_hbm, out_ref, wu_ref, tok_ref, gain_ref, rt_ref, sems, *, experts, slots
):
    copies = start_all(((rt_hbm, rt_ref), (tok_hbm, tok_ref), (gain_hbm, gain_ref), (wu_hbm, wu_ref)), sems)
    for c in copies[:3]:
        c.wait()
    toks = tok_ref.shape[0]
    xf = tok_ref[...].astype(F32)
    var = jnp.mean(xf * xf, axis=-1, keepdims=True)
    normed = (xf * lax.rsqrt(var + EPS) * gain_ref[...]).astype(BF)
    e_of = iota((experts, toks), 0)
    chosen = jnp.zeros((experts, toks), F32)
    for k in range(rt_ref.shape[0]):
        chosen = chosen + (e_of == rt_ref[k : k + 1, :]).astype(F32)
    place = slot_of(chosen, lane_ref[0], slots).astype(BF)
    n = slots * experts
    e_row = div_const(iota((n, experts), 0), slots)
    r = iota((n, toks), 0)
    slot = (r - div_const(r, slots) * slots).astype(F32)
    one = bf(dot(bf(iota((n, experts), 1) == e_row), place) == slot)
    out_ref[...] = dot(one, normed).astype(BF).reshape(out_ref.shape)
    copies[3].wait()


def hidden_units(rows, wg_ref, wu_ref, hid_ref):
    for n in range(hid_ref.shape[1] // 128):
        cols = slice(n * 128, (n + 1) * 128)
        both = dot(rows, jnp.concatenate([wg_ref[:, cols], wu_ref[:, cols]], axis=1))
        g, u = both[:, :128], both[:, 128:]
        hid_ref[:, cols] = ((0.5 * g) * (1.0 + jnp.tanh(0.5 * g)) * u).astype(BF)


def own_body(x_ref, wg_ref, wu_ref, wd_hbm, out_ref, wd_ref, hid_ref, sems):
    (copy,) = start_all(((wd_hbm, wd_ref),), sems)
    hidden_units(flat(x_ref), wg_ref, wu_ref, hid_ref)
    copy.wait()
    out_ref[...] = dot(hid_ref[...], wd_ref[...]).astype(BF)


def other_body(
    lane_ref, x_ref, wg_ref, wu_ref, wd_ref, rt_ref, gt_ref, out_ref, mix_ref, hid_ref, *, slots, experts
):
    table(lane_ref, rt_ref[...], gt_ref[...], mix_ref, slots, experts)
    hidden_units(flat(x_ref), wg_ref, wu_ref, hid_ref)
    out_ref[...] = dot(hid_ref[...], wd_ref[...]).astype(BF)


def table(lane_ref, rt, gt, mix_ref, slots, experts):
    top, toks = rt.shape
    e_of = iota((experts, toks), 0)
    chosen = jnp.zeros((experts, toks), F32)
    gate = jnp.zeros((experts, toks), F32)
    for k in range(top):
        hit = e_of == rt[k : k + 1, :]
        chosen = chosen + hit.astype(F32)
        gate = gate + jnp.where(hit, gt[k : k + 1, :], 0.0)
    place = slot_of(chosen, 1 - lane_ref[0], slots).T.astype(BF)
    gate = gate.T
    g1 = gate.astype(BF)
    rest = gate - g1.astype(F32)
    g2 = rest.astype(BF)
    g3 = (rest - g2.astype(F32)).astype(BF)
    n = slots * experts
    r = iota((1, n), 1)
    e_r = div_const(r, slots)
    slot = (r - e_r * slots).astype(F32)
    rep = bf(iota((experts, n), 0) == e_r)
    here = dot(place, rep) == slot
    for i, piece in enumerate((g1, g2, g3)):
        mix_ref[i * toks : (i + 1) * toks, :] = jnp.where(here, dot(piece, rep), 0.0).astype(BF)


def add_body(a_ref, b_ref, out_ref):
    total = a_ref[...].astype(F32) + b_ref[...].astype(F32)
    out_ref[...] = total.astype(BF).reshape(out_ref.shape)


def last_body(mix_ref, back_ref, out_ref):
    toks = out_ref.shape[0]
    s = dot(mix_ref[...], flat(back_ref))
    out_ref[...] = s[:toks] + s[toks : 2 * toks] + s[2 * toks :]


def per_device(tokens, routes, gates, norm_gain, w_gate, w_up, w_down):
    toks, width = tokens.shape
    top = routes.shape[1]
    experts = lax.axis_size("ep")
    cap = max(2, min(toks, 3 * toks * top // experts))
    slots = -(-cap // 4) * 2
    ff = w_gate.shape[2]
    items = experts * slots
    pairs = pltpu.VMEM((items // 2, 2, width), BF)
    tall = pltpu.VMEM((items, width), BF)
    swap = lambda v: lax.ppermute(v, "tp", [(0, 1), (1, 0)])
    lanes = lax.axis_index("tp").astype(jnp.int32).reshape(1)
    in_hbm = lambda *vs: [pltpu.with_memory_space_constraint(v, pltpu.HBM) for v in vs]
    wg, wu, wd = w_gate[0], w_up[0], w_down[0]
    rt = routes.T

    outgoing, wu = call(
        functools.partial(prep_body, experts=experts, slots=slots),
        (pairs, pltpu.VMEM(wu.shape, BF)),
        [SMEM] + [HBM] * 4,
        [
            pltpu.VMEM((toks, width), BF),
            pltpu.VMEM((1, width), F32),
            pltpu.VMEM((top, toks), jnp.int32),
            pltpu.SemaphoreType.DMA((4,)),
        ],
        flops=2 * items * toks * width,
    )(lanes, *in_hbm(tokens, norm_gain.reshape(1, width), rt, wu))
    exchange = lambda v: lax.all_to_all(
        v.reshape(experts, slots // 2, 2, width), "ep", split_axis=0, concat_axis=0, tiled=True
    ).reshape(v.shape)
    mine = exchange(outgoing)
    other = swap(mine)
    work = 2 * items * width * 3 * ff
    held = pltpu.VMEM((items, ff), BF)
    sent, wd = call(
        own_body, (tall, pltpu.VMEM(wd.shape, BF)), [VMEM] * 3 + [HBM],
        [held, pltpu.SemaphoreType.DMA((1,))], flops=work,
    )(mine, wg, wu, *in_hbm(wd))
    got = swap(sent)
    kept, mix = call(
        functools.partial(other_body, slots=slots, experts=experts),
        (tall, pltpu.VMEM((3 * toks, items), BF)), [SMEM] + [VMEM] * 6, [held], flops=work,
    )(lanes, other, wg, wu, wd, rt, gates.T)
    back = exchange(call(add_body, pairs, [VMEM] * 2, flops=items * width)(kept, got))
    part = call(
        last_body, pltpu.VMEM((toks, width), F32), [VMEM] * 2, flops=2 * 3 * toks * items * width
    )(mix, back)
    return (part + swap(part)).astype(BF)


def solution(mesh):
    return jax.shard_map(
        per_device,
        mesh=mesh,
        in_specs=(
            P(("grp", "ep"), None),
            P(("grp", "ep"), None),
            P(("grp", "ep"), None),
            P(),
            P("ep", None, "tp"),
            P("ep", None, "tp"),
            P("ep", "tp", None),
        ),
        out_specs=P(("grp", "ep"), None),
        check_vma=False,
    )
```

```python
import functools
import math

import jax
import jax.numpy as jnp
from jax import lax
from jax.experimental import pallas as pl
from jax.experimental.pallas import tpu as pltpu
from jax.sharding import PartitionSpec as P

EPS = 1e-06
BF = jnp.bfloat16
F32 = jnp.float32
VMEM = pl.BlockSpec(memory_space=pltpu.VMEM)
SMEM = pl.BlockSpec(memory_space=pltpu.SMEM)
HBM = pl.BlockSpec(memory_space=pltpu.HBM)
LIMIT = 16 * 1024 * 1024


def dot(a, b):
    return jnp.dot(a, b, preferred_element_type=F32)


def iota(shape, dim):
    return lax.broadcasted_iota(jnp.int32, shape, dim)


def div_const(x, n):
    return (x * (-(-(1 << 17) // n))) >> 17


def bf(mask):
    return jnp.where(mask, 1.0, 0.0).astype(BF)


def flat(ref):
    pairs, two, width = ref.shape
    return ref[...].reshape(pairs * two, width)


def call(body, outs, in_specs, scratch=(), flops=0):
    return pl.pallas_call(
        body,
        out_shape=outs,
        in_specs=in_specs,
        out_specs=jax.tree.map(lambda _: VMEM, outs),
        scratch_shapes=list(scratch),
        compiler_params=pltpu.CompilerParams(vmem_limit_bytes=LIMIT),
        cost_estimate=pl.CostEstimate(flops=flops, bytes_accessed=0, transcendentals=0),
    )


def start_all(pairs, sems):
    copies = [pltpu.make_async_copy(a, b, sems.at[i]) for i, (a, b) in enumerate(pairs)]
    for c in copies:
        c.start()
    return copies


def slot_of(chosen, core, slots):
    toks = chosen.shape[1]
    upper = bf(iota((toks, toks), 0) < iota((toks, toks), 1))
    rel = dot(chosen.astype(BF), upper) - (core * slots).astype(F32)
    return jnp.where((chosen > 0) & (rel >= 0) & (rel < slots), rel, -1.0)


def expert_at(place, core, side):
    row = place >> (side.bit_length() - 1)
    return jnp.where(core == 0, place, (place - row * side) * side + row)


def prep_body(
    lane_ref, tok_hbm, gain_hbm, rt_hbm, wu_hbm, out_ref, wu_ref, tok_ref, gain_ref, rt_ref, sems, *, experts, slots, side
):
    copies = start_all(((rt_hbm, rt_ref), (tok_hbm, tok_ref), (gain_hbm, gain_ref), (wu_hbm, wu_ref)), sems)
    for c in copies[:3]:
        c.wait()
    toks = tok_ref.shape[0]
    xf = tok_ref[...].astype(F32)
    var = jnp.mean(xf * xf, axis=-1, keepdims=True)
    normed = (xf * lax.rsqrt(var + EPS) * gain_ref[...]).astype(BF)
    e_of = iota((experts, toks), 0)
    chosen = jnp.zeros((experts, toks), F32)
    for k in range(rt_ref.shape[0]):
        chosen = chosen + (e_of == rt_ref[k : k + 1, :]).astype(F32)
    place = slot_of(chosen, lane_ref[0], slots).astype(BF)
    n = slots * experts
    e_row = expert_at(div_const(iota((n, experts), 0), slots), lane_ref[0], side)
    r = iota((n, toks), 0)
    slot = (r - div_const(r, slots) * slots).astype(F32)
    one = bf(dot(bf(iota((n, experts), 1) == e_row), place) == slot)
    out_ref[...] = dot(one, normed).astype(BF).reshape(out_ref.shape)
    copies[3].wait()


def hidden_units(rows, wg_ref, wu_ref, hid_ref):
    for n in range(hid_ref.shape[1] // 128):
        cols = slice(n * 128, (n + 1) * 128)
        both = dot(rows, jnp.concatenate([wg_ref[:, cols], wu_ref[:, cols]], axis=1))
        g, u = both[:, :128], both[:, 128:]
        hid_ref[:, cols] = ((0.5 * g) * (1.0 + jnp.tanh(0.5 * g)) * u).astype(BF)


def own_body(x_ref, wg_ref, wu_ref, wd_hbm, out_ref, wd_ref, hid_ref, sems):
    (copy,) = start_all(((wd_hbm, wd_ref),), sems)
    hidden_units(flat(x_ref), wg_ref, wu_ref, hid_ref)
    copy.wait()
    out_ref[...] = dot(hid_ref[...], wd_ref[...]).astype(BF)


def other_body(
    lane_ref, x_ref, wg_ref, wu_ref, wd_ref, rt_ref, gt_ref, out_ref, mix_ref, hid_ref, *, slots, experts, side
):
    table(lane_ref, rt_ref[...], gt_ref[...], mix_ref, slots, experts, side)
    hidden_units(flat(x_ref), wg_ref, wu_ref, hid_ref)
    out_ref[...] = dot(hid_ref[...], wd_ref[...]).astype(BF)


def table(lane_ref, rt, gt, mix_ref, slots, experts, side):
    top, toks = rt.shape
    e_of = iota((experts, toks), 0)
    chosen = jnp.zeros((experts, toks), F32)
    gate = jnp.zeros((experts, toks), F32)
    for k in range(top):
        hit = e_of == rt[k : k + 1, :]
        chosen = chosen + hit.astype(F32)
        gate = gate + jnp.where(hit, gt[k : k + 1, :], 0.0)
    place = slot_of(chosen, 1 - lane_ref[0], slots).T.astype(BF)
    gate = gate.T
    g1 = gate.astype(BF)
    rest = gate - g1.astype(F32)
    g2 = rest.astype(BF)
    g3 = (rest - g2.astype(F32)).astype(BF)
    n = slots * experts
    r = iota((1, n), 1)
    e_r = div_const(r, slots)
    slot = (r - e_r * slots).astype(F32)
    rep = bf(iota((experts, n), 0) == expert_at(e_r, 1 - lane_ref[0], side))
    here = dot(place, rep) == slot
    for i, piece in enumerate((g1, g2, g3)):
        mix_ref[i * toks : (i + 1) * toks, :] = jnp.where(here, dot(piece, rep), 0.0).astype(BF)


def add_body(a_ref, b_ref, out_ref):
    total = a_ref[...].astype(F32) + b_ref[...].astype(F32)
    out_ref[...] = total.astype(BF).reshape(out_ref.shape)


def last_body(mix_ref, back_ref, out_ref):
    toks = out_ref.shape[0]
    s = dot(mix_ref[...], flat(back_ref))
    out_ref[...] = s[:toks] + s[toks : 2 * toks] + s[2 * toks :]


def per_device(tokens, routes, gates, norm_gain, w_gate, w_up, w_down):
    toks, width = tokens.shape
    top = routes.shape[1]
    experts = lax.axis_size("ep")
    cap = max(2, min(toks, 3 * toks * top // experts))
    slots = -(-cap // 4) * 2
    ff = w_gate.shape[2]
    side = math.isqrt(experts)
    items = experts * slots
    pairs = pltpu.VMEM((items // 2, 2, width), BF)
    tall = pltpu.VMEM((items, width), BF)
    swap = lambda v: lax.ppermute(v, "tp", [(0, 1), (1, 0)])
    lanes = lax.axis_index("tp").astype(jnp.int32).reshape(1)
    in_hbm = lambda *vs: [pltpu.with_memory_space_constraint(v, pltpu.HBM) for v in vs]
    wg, wu, wd = w_gate[0], w_up[0], w_down[0]
    rt = routes.T

    outgoing, wu = call(
        functools.partial(prep_body, experts=experts, slots=slots, side=side),
        (pairs, pltpu.VMEM(wu.shape, BF)),
        [SMEM] + [HBM] * 4,
        [
            pltpu.VMEM((toks, width), BF),
            pltpu.VMEM((1, width), F32),
            pltpu.VMEM((top, toks), jnp.int32),
            pltpu.SemaphoreType.DMA((4,)),
        ],
        flops=2 * items * toks * width,
    )(lanes, *in_hbm(tokens, norm_gain.reshape(1, width), rt, wu))
    by_row = list(range(experts))
    by_column = [(p % side) * side + p // side for p in by_row]

    def exchange(v, first, second):
        return lax.all_to_all(
            v.reshape(experts, slots // 2, 2, width), ("ep", "tp"), split_axis=0, concat_axis=0, tiled=True,
            axis_index_groups=[[2 * e for e in first], [2 * e + 1 for e in second]],
        ).reshape(v.shape)

    mine = exchange(outgoing, by_row, by_column)
    other = swap(mine)
    work = 2 * items * width * 3 * ff
    held = pltpu.VMEM((items, ff), BF)
    sent, wd = call(
        own_body, (tall, pltpu.VMEM(wd.shape, BF)), [VMEM] * 3 + [HBM],
        [held, pltpu.SemaphoreType.DMA((1,))], flops=work,
    )(mine, wg, wu, *in_hbm(wd))
    got = swap(sent)
    kept, mix = call(
        functools.partial(other_body, slots=slots, experts=experts, side=side),
        (tall, pltpu.VMEM((3 * toks, items), BF)), [SMEM] + [VMEM] * 6, [held], flops=work,
    )(lanes, other, wg, wu, wd, rt, gates.T)
    back = exchange(call(add_body, pairs, [VMEM] * 2, flops=items * width)(kept, got), by_column, by_row)
    part = call(
        last_body, pltpu.VMEM((toks, width), F32), [VMEM] * 2, flops=2 * 3 * toks * items * width
    )(mix, back)
    return (part + swap(part)).astype(BF)


def solution(mesh):
    return jax.shard_map(
        per_device,
        mesh=mesh,
        in_specs=(
            P(("grp", "ep"), None),
            P(("grp", "ep"), None),
            P(("grp", "ep"), None),
            P(),
            P("ep", None, "tp"),
            P("ep", None, "tp"),
            P("ep", "tp", None),
        ),
        out_specs=P(("grp", "ep"), None),
        check_vma=False,
    )
```

```python
import functools

import jax
import jax.numpy as jnp
from jax import lax
from jax.experimental import pallas as pl
from jax.experimental.pallas import tpu as pltpu
from jax.sharding import PartitionSpec as P

EPS = 1e-06
BF = jnp.bfloat16
F32 = jnp.float32
VMEM = pl.BlockSpec(memory_space=pltpu.VMEM)
SMEM = pl.BlockSpec(memory_space=pltpu.SMEM)
HBM = pl.BlockSpec(memory_space=pltpu.HBM)
LIMIT = 16 * 1024 * 1024


def dot(a, b):
    return jnp.dot(a, b, preferred_element_type=F32)


def iota(shape, dim):
    return lax.broadcasted_iota(jnp.int32, shape, dim)


def div_const(x, n):
    return (x * (-(-(1 << 17) // n))) >> 17


def bf(mask):
    return jnp.where(mask, 1.0, 0.0).astype(BF)


def flat(ref):
    pairs, two, width = ref.shape
    return ref[...].reshape(pairs * two, width)


def call(body, outs, in_specs, scratch=(), flops=0):
    return pl.pallas_call(
        body,
        out_shape=outs,
        in_specs=in_specs,
        out_specs=jax.tree.map(lambda _: VMEM, outs),
        scratch_shapes=list(scratch),
        compiler_params=pltpu.CompilerParams(vmem_limit_bytes=LIMIT),
        cost_estimate=pl.CostEstimate(flops=flops, bytes_accessed=0, transcendentals=0),
    )


def start_all(pairs, sems):
    copies = [pltpu.make_async_copy(a, b, sems.at[i]) for i, (a, b) in enumerate(pairs)]
    for c in copies:
        c.start()
    return copies


def slot_of(chosen, core, slots):
    toks = chosen.shape[1]
    upper = bf(iota((toks, toks), 0) < iota((toks, toks), 1))
    rel = dot(chosen.astype(BF), upper) - (core * slots).astype(F32)
    return jnp.where((chosen > 0) & (rel >= 0) & (rel < slots), rel, -1.0)


def prep_body(
    lane_ref, tok_hbm, gain_hbm, rt_hbm, gt_hbm, wu_hbm,
    out_ref, wu_ref, mix_ref,
    tok_ref, gain_ref, rt_ref, gt_ref, sems, *, experts, slots,
):
    copies = start_all(
        ((rt_hbm, rt_ref), (tok_hbm, tok_ref), (gain_hbm, gain_ref), (gt_hbm, gt_ref), (wu_hbm, wu_ref)), sems
    )
    for c in copies[:4]:
        c.wait()
    toks = tok_ref.shape[0]
    xf = tok_ref[...].astype(F32)
    var = jnp.mean(xf * xf, axis=-1, keepdims=True)
    normed = (xf * lax.rsqrt(var + EPS) * gain_ref[...]).astype(BF)
    e_of = iota((experts, toks), 0)
    chosen = jnp.zeros((experts, toks), F32)
    for k in range(rt_ref.shape[0]):
        chosen = chosen + (e_of == rt_ref[k : k + 1, :]).astype(F32)
    place = slot_of(chosen, lane_ref[0], slots).astype(BF)
    n = slots * experts
    e_row = div_const(iota((n, experts), 0), slots)
    r = iota((n, toks), 0)
    slot = (r - div_const(r, slots) * slots).astype(F32)
    one = bf(dot(bf(iota((n, experts), 1) == e_row), place) == slot)
    out_ref[...] = dot(one, normed).astype(BF).reshape(out_ref.shape)
    table(lane_ref, rt_ref[...], gt_ref[...], mix_ref, slots, experts)
    copies[4].wait()


def hidden_units(rows, wg_ref, wu_ref, hid_ref):
    for n in range(hid_ref.shape[1] // 128):
        cols = slice(n * 128, (n + 1) * 128)
        both = dot(rows, jnp.concatenate([wg_ref[:, cols], wu_ref[:, cols]], axis=1))
        g, u = both[:, :128], both[:, 128:]
        hid_ref[:, cols] = ((0.5 * g) * (1.0 + jnp.tanh(0.5 * g)) * u).astype(BF)


def own_body(x_ref, wg_ref, wu_ref, wd_hbm, out_ref, wd_ref, hid_ref, sems):
    (copy,) = start_all(((wd_hbm, wd_ref),), sems)
    hidden_units(flat(x_ref), wg_ref, wu_ref, hid_ref)
    copy.wait()
    out_ref[...] = dot(hid_ref[...], wd_ref[...]).astype(BF)


def other_body(x_ref, wg_ref, wu_ref, wd_ref, out_ref, hid_ref):
    hidden_units(flat(x_ref), wg_ref, wu_ref, hid_ref)
    out_ref[...] = dot(hid_ref[...], wd_ref[...]).astype(BF)


def table(lane_ref, rt, gt, mix_ref, slots, experts):
    top, toks = rt.shape
    e_of = iota((experts, toks), 0)
    chosen = jnp.zeros((experts, toks), F32)
    gate = jnp.zeros((experts, toks), F32)
    for k in range(top):
        hit = e_of == rt[k : k + 1, :]
        chosen = chosen + hit.astype(F32)
        gate = gate + jnp.where(hit, gt[k : k + 1, :], 0.0)
    place = slot_of(chosen, 1 - lane_ref[0], slots).T.astype(BF)
    gate = gate.T
    g1 = gate.astype(BF)
    rest = gate - g1.astype(F32)
    g2 = rest.astype(BF)
    g3 = (rest - g2.astype(F32)).astype(BF)
    n = slots * experts
    r = iota((1, n), 1)
    e_r = div_const(r, slots)
    slot = (r - e_r * slots).astype(F32)
    rep = bf(iota((experts, n), 0) == e_r)
    here = dot(place, rep) == slot
    for i, piece in enumerate((g1, g2, g3)):
        mix_ref[i * toks : (i + 1) * toks, :] = jnp.where(here, dot(piece, rep), 0.0).astype(BF)


def add_body(a_ref, b_ref, out_ref):
    total = a_ref[...].astype(F32) + b_ref[...].astype(F32)
    out_ref[...] = total.astype(BF).reshape(out_ref.shape)


def last_body(mix_ref, back_ref, out_ref):
    toks = out_ref.shape[0]
    s = dot(mix_ref[...], flat(back_ref))
    out_ref[...] = s[:toks] + s[toks : 2 * toks] + s[2 * toks :]


def per_device(tokens, routes, gates, norm_gain, w_gate, w_up, w_down):
    toks, width = tokens.shape
    top = routes.shape[1]
    experts = lax.axis_size("ep")
    cap = max(2, min(toks, 3 * toks * top // experts))
    slots = -(-cap // 4) * 2
    ff = w_gate.shape[2]
    items = experts * slots
    pairs = pltpu.VMEM((items // 2, 2, width), BF)
    tall = pltpu.VMEM((items, width), BF)
    swap = lambda v: lax.ppermute(v, "tp", [(0, 1), (1, 0)])
    lanes = lax.axis_index("tp").astype(jnp.int32).reshape(1)
    in_hbm = lambda *vs: [pltpu.with_memory_space_constraint(v, pltpu.HBM) for v in vs]
    wg, wu, wd = w_gate[0], w_up[0], w_down[0]

    outgoing, wu, mix = call(
        functools.partial(prep_body, experts=experts, slots=slots),
        (pairs, pltpu.VMEM(wu.shape, BF), pltpu.VMEM((3 * toks, items), BF)),
        [SMEM] + [HBM] * 5,
        [
            pltpu.VMEM((toks, width), BF),
            pltpu.VMEM((1, width), F32),
            pltpu.VMEM((top, toks), jnp.int32),
            pltpu.VMEM((top, toks), F32),
            pltpu.SemaphoreType.DMA((5,)),
        ],
        flops=2 * items * toks * width,
    )(lanes, *in_hbm(tokens, norm_gain.reshape(1, width), routes.T, gates.T, wu))
    exchange = lambda v: lax.all_to_all(
        v.reshape(experts, slots // 2, 2, width), "ep", split_axis=0, concat_axis=0, tiled=True
    ).reshape(v.shape)
    mine = exchange(outgoing)
    other = swap(mine)
    work = 2 * items * width * 3 * ff
    held = pltpu.VMEM((items, ff), BF)
    sent, wd = call(
        own_body, (tall, pltpu.VMEM(wd.shape, BF)), [VMEM] * 3 + [HBM],
        [held, pltpu.SemaphoreType.DMA((1,))], flops=work,
    )(mine, wg, wu, *in_hbm(wd))
    got = swap(sent)
    kept = call(other_body, tall, [VMEM] * 4, [held], flops=work)(other, wg, wu, wd)
    back = exchange(call(add_body, pairs, [VMEM] * 2, flops=items * width)(kept, got))
    part = call(
        last_body, pltpu.VMEM((toks, width), F32), [VMEM] * 2, flops=2 * 3 * toks * items * width
    )(mix, back)
    return (part + swap(part)).astype(BF)


def solution(mesh):
    return jax.shard_map(
        per_device,
        mesh=mesh,
        in_specs=(
            P(("grp", "ep"), None),
            P(("grp", "ep"), None),
            P(("grp", "ep"), None),
            P(),
            P("ep", None, "tp"),
            P("ep", None, "tp"),
            P("ep", "tp", None),
        ),
        out_specs=P(("grp", "ep"), None),
        check_vma=False,
    )
```

```python
import functools

import jax
import jax.numpy as jnp
from jax import lax
from jax.experimental import pallas as pl
from jax.experimental.pallas import tpu as pltpu
from jax.sharding import PartitionSpec as P

EPS = 1e-06
BF = jnp.bfloat16
F32 = jnp.float32
VMEM = pl.BlockSpec(memory_space=pltpu.VMEM)
SMEM = pl.BlockSpec(memory_space=pltpu.SMEM)
HBM = pl.BlockSpec(memory_space=pltpu.HBM)
HEAD_START = 1500
LIMIT = 16 * 1024 * 1024


def dot(a, b):
    return jnp.dot(a, b, preferred_element_type=F32)


def iota(shape, dim):
    return lax.broadcasted_iota(jnp.int32, shape, dim)


def div_const(x, n):
    return (x * (-(-(1 << 17) // n))) >> 17


def bf(mask):
    return jnp.where(mask, 1.0, 0.0).astype(BF)


def flat(ref):
    pairs, two, width = ref.shape
    return ref[...].reshape(pairs * two, width)


def call(body, outs, in_specs, scratch=(), flops=0):
    return pl.pallas_call(
        body,
        out_shape=outs,
        in_specs=in_specs,
        out_specs=jax.tree.map(lambda _: VMEM, outs),
        scratch_shapes=list(scratch),
        compiler_params=pltpu.CompilerParams(vmem_limit_bytes=LIMIT),
        cost_estimate=pl.CostEstimate(flops=flops, bytes_accessed=0, transcendentals=0),
    )


def start_all(pairs, sems):
    copies = [pltpu.make_async_copy(a, b, sems.at[i]) for i, (a, b) in enumerate(pairs)]
    for c in copies:
        c.start()
    return copies


def slot_of(chosen, core, slots):
    toks = chosen.shape[1]
    upper = bf(iota((toks, toks), 0) < iota((toks, toks), 1))
    rel = dot(chosen.astype(BF), upper) - (core * slots).astype(F32)
    return jnp.where((chosen > 0) & (rel >= 0) & (rel < slots), rel, -1.0)


def prep_body(
    lane_ref, tok_hbm, gain_hbm, rt_hbm, gt_hbm, wu_hbm,
    out_ref, wu_ref, mix_ref,
    tok_ref, gain_ref, rt_ref, gt_ref, sems, *, experts, slots,
):
    copies = start_all(
        ((rt_hbm, rt_ref), (tok_hbm, tok_ref), (gain_hbm, gain_ref), (gt_hbm, gt_ref), (wu_hbm, wu_ref)), sems
    )
    for c in copies[:4]:
        c.wait()
    toks = tok_ref.shape[0]
    xf = tok_ref[...].astype(F32)
    var = jnp.mean(xf * xf, axis=-1, keepdims=True)
    normed = (xf * lax.rsqrt(var + EPS) * gain_ref[...]).astype(BF)
    e_of = iota((experts, toks), 0)
    chosen = jnp.zeros((experts, toks), F32)
    for k in range(rt_ref.shape[0]):
        chosen = chosen + (e_of == rt_ref[k : k + 1, :]).astype(F32)
    place = slot_of(chosen, lane_ref[0], slots).astype(BF)
    n = slots * experts
    e_row = div_const(iota((n, experts), 0), slots)
    r = iota((n, toks), 0)
    slot = (r - div_const(r, slots) * slots).astype(F32)
    one = bf(dot(bf(iota((n, experts), 1) == e_row), place) == slot)
    out_ref[...] = dot(one, normed).astype(BF).reshape(out_ref.shape)
    table(lane_ref, rt_ref[...], gt_ref[...], mix_ref, slots, experts)
    copies[4].wait()


def hidden_units(rows, wg_ref, wu_ref, hid_ref):
    for n in range(hid_ref.shape[1] // 128):
        cols = slice(n * 128, (n + 1) * 128)
        both = dot(rows, jnp.concatenate([wg_ref[:, cols], wu_ref[:, cols]], axis=1))
        g, u = both[:, :128], both[:, 128:]
        hid_ref[:, cols] = ((0.5 * g) * (1.0 + jnp.tanh(0.5 * g)) * u).astype(BF)


def own_body(x_ref, wg_ref, wu_ref, wd_hbm, out_ref, wd_ref, hid_ref, sems):
    (copy,) = start_all(((wd_hbm, wd_ref),), sems)
    hidden_units(flat(x_ref), wg_ref, wu_ref, hid_ref)
    copy.wait()
    out_ref[...] = dot(hid_ref[...], wd_ref[...]).astype(BF)


def other_body(x_ref, wg_ref, wu_ref, wd_ref, out_ref, hid_ref):
    hidden_units(flat(x_ref), wg_ref, wu_ref, hid_ref)
    out_ref[...] = dot(hid_ref[...], wd_ref[...]).astype(BF)


def table(lane_ref, rt, gt, mix_ref, slots, experts):
    top, toks = rt.shape
    e_of = iota((experts, toks), 0)
    chosen = jnp.zeros((experts, toks), F32)
    gate = jnp.zeros((experts, toks), F32)
    for k in range(top):
        hit = e_of == rt[k : k + 1, :]
        chosen = chosen + hit.astype(F32)
        gate = gate + jnp.where(hit, gt[k : k + 1, :], 0.0)
    place = slot_of(chosen, 1 - lane_ref[0], slots).T.astype(BF)
    gate = gate.T
    g1 = gate.astype(BF)
    rest = gate - g1.astype(F32)
    g2 = rest.astype(BF)
    g3 = (rest - g2.astype(F32)).astype(BF)
    n = slots * experts
    r = iota((1, n), 1)
    e_r = div_const(r, slots)
    slot = (r - e_r * slots).astype(F32)
    rep = bf(iota((experts, n), 0) == e_r)
    here = dot(place, rep) == slot
    for i, piece in enumerate((g1, g2, g3)):
        mix_ref[i * toks : (i + 1) * toks, :] = jnp.where(here, dot(piece, rep), 0.0).astype(BF)


def add_body(lane_ref, a_ref, b_ref, out_ref):
    total = a_ref[...].astype(F32) + b_ref[...].astype(F32)
    out_ref[...] = total.astype(BF).reshape(out_ref.shape)

    @pl.when(lane_ref[0] == 1)
    def _():
        pl.delay(HEAD_START)


def last_body(mix_ref, back_ref, out_ref):
    toks = out_ref.shape[0]
    s = dot(mix_ref[...], flat(back_ref))
    out_ref[...] = s[:toks] + s[toks : 2 * toks] + s[2 * toks :]


def per_device(tokens, routes, gates, norm_gain, w_gate, w_up, w_down):
    toks, width = tokens.shape
    top = routes.shape[1]
    experts = lax.axis_size("ep")
    cap = max(2, min(toks, 3 * toks * top // experts))
    slots = -(-cap // 4) * 2
    ff = w_gate.shape[2]
    items = experts * slots
    pairs = pltpu.VMEM((items // 2, 2, width), BF)
    tall = pltpu.VMEM((items, width), BF)
    swap = lambda v: lax.ppermute(v, "tp", [(0, 1), (1, 0)])
    lanes = lax.axis_index("tp").astype(jnp.int32).reshape(1)
    in_hbm = lambda *vs: [pltpu.with_memory_space_constraint(v, pltpu.HBM) for v in vs]
    wg, wu, wd = w_gate[0], w_up[0], w_down[0]

    outgoing, wu, mix = call(
        functools.partial(prep_body, experts=experts, slots=slots),
        (pairs, pltpu.VMEM(wu.shape, BF), pltpu.VMEM((3 * toks, items), BF)),
        [SMEM] + [HBM] * 5,
        [
            pltpu.VMEM((toks, width), BF),
            pltpu.VMEM((1, width), F32),
            pltpu.VMEM((top, toks), jnp.int32),
            pltpu.VMEM((top, toks), F32),
            pltpu.SemaphoreType.DMA((5,)),
        ],
        flops=2 * items * toks * width,
    )(lanes, *in_hbm(tokens, norm_gain.reshape(1, width), routes.T, gates.T, wu))
    exchange = lambda v: lax.all_to_all(
        v.reshape(experts, slots // 2, 2, width), "ep", split_axis=0, concat_axis=0, tiled=True
    ).reshape(v.shape)
    mine = exchange(outgoing)
    other = swap(mine)
    work = 2 * items * width * 3 * ff
    held = pltpu.VMEM((items, ff), BF)
    sent, wd = call(
        own_body, (tall, pltpu.VMEM(wd.shape, BF)), [VMEM] * 3 + [HBM],
        [held, pltpu.SemaphoreType.DMA((1,))], flops=work,
    )(mine, wg, wu, *in_hbm(wd))
    got = swap(sent)
    kept = call(other_body, tall, [VMEM] * 4, [held], flops=work)(other, wg, wu, wd)
    back = exchange(call(add_body, pairs, [SMEM] + [VMEM] * 2, flops=items * width)(lanes, kept, got))
    part = call(
        last_body, pltpu.VMEM((toks, width), F32), [VMEM] * 2, flops=2 * 3 * toks * items * width
    )(mix, back)
    return (part + swap(part)).astype(BF)


def solution(mesh):
    return jax.shard_map(
        per_device,
        mesh=mesh,
        in_specs=(
            P(("grp", "ep"), None),
            P(("grp", "ep"), None),
            P(("grp", "ep"), None),
            P(),
            P("ep", None, "tp"),
            P("ep", None, "tp"),
            P("ep", "tp", None),
        ),
        out_specs=P(("grp", "ep"), None),
        check_vma=False,
    )
```

```python
import functools

import jax
import jax.numpy as jnp
from jax import lax
from jax.experimental import pallas as pl
from jax.experimental.pallas import tpu as pltpu
from jax.sharding import PartitionSpec as P

EPS = 1e-06
BF = jnp.bfloat16
F32 = jnp.float32
VMEM = pl.BlockSpec(memory_space=pltpu.VMEM)
SMEM = pl.BlockSpec(memory_space=pltpu.SMEM)
HBM = pl.BlockSpec(memory_space=pltpu.HBM)
LIMIT = 16 * 1024 * 1024


def dot(a, b):
    return jnp.dot(a, b, preferred_element_type=F32)


def iota(shape, dim):
    return lax.broadcasted_iota(jnp.int32, shape, dim)


def div_const(x, n):
    return (x * (-(-(1 << 17) // n))) >> 17


def bf(mask):
    return jnp.where(mask, 1.0, 0.0).astype(BF)


def flat(ref):
    pairs, two, width = ref.shape
    return ref[...].reshape(pairs * two, width)


def call(body, outs, in_specs, scratch=(), flops=0):
    return pl.pallas_call(
        body,
        out_shape=outs,
        in_specs=in_specs,
        out_specs=jax.tree.map(lambda _: VMEM, outs),
        scratch_shapes=list(scratch),
        compiler_params=pltpu.CompilerParams(vmem_limit_bytes=LIMIT),
        cost_estimate=pl.CostEstimate(flops=flops, bytes_accessed=0, transcendentals=0),
    )


def start_all(pairs, sems, urgent=0):
    copies = [pltpu.make_async_copy(a, b, sems.at[i]) for i, (a, b) in enumerate(pairs)]
    for i, c in enumerate(copies):
        c.start(priority=int(i < urgent))
    return copies


def slot_of(chosen, core, slots):
    toks = chosen.shape[1]
    upper = bf(iota((toks, toks), 0) < iota((toks, toks), 1))
    rel = dot(chosen.astype(BF), upper) - (core * slots).astype(F32)
    return jnp.where((chosen > 0) & (rel >= 0) & (rel < slots), rel, -1.0)


def prep_body(
    lane_ref, tok_hbm, gain_hbm, rt_hbm, gt_hbm, wu_hbm,
    out_ref, wu_ref, mix_ref,
    tok_ref, gain_ref, rt_ref, gt_ref, sems, *, experts, slots,
):
    pairs = ((rt_hbm, rt_ref), (gt_hbm, gt_ref), (tok_hbm, tok_ref), (gain_hbm, gain_ref), (wu_hbm, wu_ref))
    copies = start_all(pairs, sems, urgent=4)
    copies[0].wait()
    copies[1].wait()
    toks = tok_ref.shape[0]
    e_of = iota((experts, toks), 0)
    chosen = jnp.zeros((experts, toks), F32)
    for k in range(rt_ref.shape[0]):
        chosen = chosen + (e_of == rt_ref[k : k + 1, :]).astype(F32)
    place = slot_of(chosen, lane_ref[0], slots).astype(BF)
    n = slots * experts
    e_row = div_const(iota((n, experts), 0), slots)
    r = iota((n, toks), 0)
    slot = (r - div_const(r, slots) * slots).astype(F32)
    one = bf(dot(bf(iota((n, experts), 1) == e_row), place) == slot)
    table(lane_ref, rt_ref[...], gt_ref[...], mix_ref, slots, experts)
    copies[2].wait()
    copies[3].wait()
    xf = tok_ref[...].astype(F32)
    var = jnp.mean(xf * xf, axis=-1, keepdims=True)
    normed = (xf * lax.rsqrt(var + EPS) * gain_ref[...]).astype(BF)
    out_ref[...] = dot(one, normed).astype(BF).reshape(out_ref.shape)
    copies[4].wait()


def hidden_units(rows, wg_ref, wu_ref, hid_ref):
    for n in range(hid_ref.shape[1] // 128):
        cols = slice(n * 128, (n + 1) * 128)
        both = dot(rows, jnp.concatenate([wg_ref[:, cols], wu_ref[:, cols]], axis=1))
        g, u = both[:, :128], both[:, 128:]
        hid_ref[:, cols] = ((0.5 * g) * (1.0 + jnp.tanh(0.5 * g)) * u).astype(BF)


def own_body(x_ref, wg_ref, wu_ref, wd_hbm, out_ref, wd_ref, hid_ref, sems):
    (copy,) = start_all(((wd_hbm, wd_ref),), sems)
    hidden_units(flat(x_ref), wg_ref, wu_ref, hid_ref)
    copy.wait()
    out_ref[...] = dot(hid_ref[...], wd_ref[...]).astype(BF)


def other_body(x_ref, wg_ref, wu_ref, wd_ref, out_ref, hid_ref):
    hidden_units(flat(x_ref), wg_ref, wu_ref, hid_ref)
    out_ref[...] = dot(hid_ref[...], wd_ref[...]).astype(BF)


def table(lane_ref, rt, gt, mix_ref, slots, experts):
    top, toks = rt.shape
    e_of = iota((experts, toks), 0)
    chosen = jnp.zeros((experts, toks), F32)
    gate = jnp.zeros((experts, toks), F32)
    for k in range(top):
        hit = e_of == rt[k : k + 1, :]
        chosen = chosen + hit.astype(F32)
        gate = gate + jnp.where(hit, gt[k : k + 1, :], 0.0)
    place = slot_of(chosen, 1 - lane_ref[0], slots).T.astype(BF)
    gate = gate.T
    g1 = gate.astype(BF)
    rest = gate - g1.astype(F32)
    g2 = rest.astype(BF)
    g3 = (rest - g2.astype(F32)).astype(BF)
    n = slots * experts
    r = iota((1, n), 1)
    e_r = div_const(r, slots)
    slot = (r - e_r * slots).astype(F32)
    rep = bf(iota((experts, n), 0) == e_r)
    here = dot(place, rep) == slot
    for i, piece in enumerate((g1, g2, g3)):
        mix_ref[i * toks : (i + 1) * toks, :] = jnp.where(here, dot(piece, rep), 0.0).astype(BF)


def add_body(a_ref, b_ref, out_ref):
    total = a_ref[...].astype(F32) + b_ref[...].astype(F32)
    out_ref[...] = total.astype(BF).reshape(out_ref.shape)


def last_body(mix_ref, back_ref, out_ref):
    toks = out_ref.shape[0]
    s = dot(mix_ref[...], flat(back_ref))
    out_ref[...] = s[:toks] + s[toks : 2 * toks] + s[2 * toks :]


def per_device(tokens, routes, gates, norm_gain, w_gate, w_up, w_down):
    toks, width = tokens.shape
    top = routes.shape[1]
    experts = lax.axis_size("ep")
    cap = max(2, min(toks, 3 * toks * top // experts))
    slots = -(-cap // 4) * 2
    ff = w_gate.shape[2]
    items = experts * slots
    pairs = pltpu.VMEM((items // 2, 2, width), BF)
    tall = pltpu.VMEM((items, width), BF)
    swap = lambda v: lax.ppermute(v, "tp", [(0, 1), (1, 0)])
    lanes = lax.axis_index("tp").astype(jnp.int32).reshape(1)
    in_hbm = lambda *vs: [pltpu.with_memory_space_constraint(v, pltpu.HBM) for v in vs]
    wg, wu, wd = w_gate[0], w_up[0], w_down[0]

    outgoing, wu, mix = call(
        functools.partial(prep_body, experts=experts, slots=slots),
        (pairs, pltpu.VMEM(wu.shape, BF), pltpu.VMEM((3 * toks, items), BF)),
        [SMEM] + [HBM] * 5,
        [
            pltpu.VMEM((toks, width), BF),
            pltpu.VMEM((1, width), F32),
            pltpu.VMEM((top, toks), jnp.int32),
            pltpu.VMEM((top, toks), F32),
            pltpu.SemaphoreType.DMA((5,)),
        ],
        flops=2 * items * toks * width,
    )(lanes, *in_hbm(tokens, norm_gain.reshape(1, width), routes.T, gates.T, wu))
    exchange = lambda v: lax.all_to_all(
        v.reshape(experts, slots // 2, 2, width), "ep", split_axis=0, concat_axis=0, tiled=True
    ).reshape(v.shape)
    mine = exchange(outgoing)
    other = swap(mine)
    work = 2 * items * width * 3 * ff
    held = pltpu.VMEM((items, ff), BF)
    sent, wd = call(
        own_body, (tall, pltpu.VMEM(wd.shape, BF)), [VMEM] * 3 + [HBM],
        [held, pltpu.SemaphoreType.DMA((1,))], flops=work,
    )(mine, wg, wu, *in_hbm(wd))
    got = swap(sent)
    kept = call(other_body, tall, [VMEM] * 4, [held], flops=work)(other, wg, wu, wd)
    back = exchange(call(add_body, pairs, [VMEM] * 2, flops=items * width)(kept, got))
    part = call(
        last_body, pltpu.VMEM((toks, width), F32), [VMEM] * 2, flops=2 * 3 * toks * items * width
    )(mix, back)
    return (part + swap(part)).astype(BF)


def solution(mesh):
    return jax.shard_map(
        per_device,
        mesh=mesh,
        in_specs=(
            P(("grp", "ep"), None),
            P(("grp", "ep"), None),
            P(("grp", "ep"), None),
            P(),
            P("ep", None, "tp"),
            P("ep", None, "tp"),
            P("ep", "tp", None),
        ),
        out_specs=P(("grp", "ep"), None),
        check_vma=False,
    )
```

```python
import functools

import jax
import jax.numpy as jnp
from jax import lax
from jax.experimental import pallas as pl
from jax.experimental.pallas import tpu as pltpu
from jax.sharding import PartitionSpec as P

EPS = 1e-06
BF = jnp.bfloat16
F32 = jnp.float32
VMEM = pl.BlockSpec(memory_space=pltpu.VMEM)
SMEM = pl.BlockSpec(memory_space=pltpu.SMEM)
HBM = pl.BlockSpec(memory_space=pltpu.HBM)
LIMIT = 16 * 1024 * 1024


def dot(a, b):
    return jnp.dot(a, b, preferred_element_type=F32)


def iota(shape, dim):
    return lax.broadcasted_iota(jnp.int32, shape, dim)


def div_const(x, n):
    return (x * (-(-(1 << 17) // n))) >> 17


def bf(mask):
    return jnp.where(mask, 1.0, 0.0).astype(BF)


def flat(ref):
    pairs, two, width = ref.shape
    return ref[...].reshape(pairs * two, width)


def call(body, outs, in_specs, scratch=(), flops=0):
    return pl.pallas_call(
        body,
        out_shape=outs,
        in_specs=in_specs,
        out_specs=jax.tree.map(lambda _: VMEM, outs),
        scratch_shapes=list(scratch),
        compiler_params=pltpu.CompilerParams(vmem_limit_bytes=LIMIT),
        cost_estimate=pl.CostEstimate(flops=flops, bytes_accessed=0, transcendentals=0),
    )


def start_all(pairs, sems):
    copies = [pltpu.make_async_copy(a, b, sems.at[i]) for i, (a, b) in enumerate(pairs)]
    for c in copies:
        c.start()
    return copies


def slot_of(chosen, core, slots):
    toks = chosen.shape[1]
    upper = bf(iota((toks, toks), 0) < iota((toks, toks), 1))
    rel = dot(chosen.astype(BF), upper) - (core * slots).astype(F32)
    return jnp.where((chosen > 0) & (rel >= 0) & (rel < slots), rel, -1.0)


def prep_body(
    lane_ref, tok_hbm, gain_hbm, rt_hbm, gt_hbm, wu_hbm,
    out_ref, wu_ref, mix_ref,
    tok_ref, gain_ref, rt_ref, gt_ref, sems, *, experts, slots,
):
    copies = start_all(
        ((rt_hbm, rt_ref), (tok_hbm, tok_ref), (gain_hbm, gain_ref), (gt_hbm, gt_ref), (wu_hbm, wu_ref)), sems
    )
    for c in copies[:4]:
        c.wait()
    toks = tok_ref.shape[0]
    xf = tok_ref[...].astype(F32)
    var = jnp.mean(xf * xf, axis=-1, keepdims=True)
    normed = (xf * lax.rsqrt(var + EPS) * gain_ref[...]).astype(BF)
    e_of = iota((experts, toks), 0)
    chosen = jnp.zeros((experts, toks), F32)
    for k in range(rt_ref.shape[0]):
        chosen = chosen + (e_of == rt_ref[k : k + 1, :]).astype(F32)
    place = slot_of(chosen, lane_ref[0], slots).astype(BF)
    n = slots * experts
    e_row = div_const(iota((n, experts), 0), slots)
    r = iota((n, toks), 0)
    slot = (r - div_const(r, slots) * slots).astype(F32)
    one = bf(dot(bf(iota((n, experts), 1) == e_row), place) == slot)
    out_ref[...] = dot(one, normed).astype(BF).reshape(out_ref.shape)
    table(lane_ref, rt_ref[...], gt_ref[...], mix_ref, slots, experts)
    copies[4].wait()


def hidden_units(rows, wg_ref, wu_ref, hid_ref):
    for n in range(hid_ref.shape[1] // 128):
        cols = slice(n * 128, (n + 1) * 128)
        both = dot(rows, jnp.concatenate([wg_ref[:, cols], wu_ref[:, cols]], axis=1))
        g, u = both[:, :128], both[:, 128:]
        hid_ref[:, cols] = ((0.5 * g) * (1.0 + jnp.tanh(0.5 * g)) * u).astype(BF)


def own_body(x_ref, wg_ref, wu_ref, wd_hbm, out_ref, wd_ref, hid_ref, sems):
    (copy,) = start_all(((wd_hbm, wd_ref),), sems)
    hidden_units(flat(x_ref), wg_ref, wu_ref, hid_ref)
    copy.wait()
    out_ref[...] = dot(hid_ref[...], wd_ref[...]).astype(BF)


def other_body(x_ref, wg_ref, wu_ref, wd_ref, out_ref, hid_ref):
    hidden_units(flat(x_ref), wg_ref, wu_ref, hid_ref)
    out_ref[...] = dot(hid_ref[...], wd_ref[...]).astype(BF)


def table(lane_ref, rt, gt, mix_ref, slots, experts):
    top, toks = rt.shape
    e_of = iota((experts, toks), 0)
    chosen = jnp.zeros((experts, toks), F32)
    gate = jnp.zeros((experts, toks), F32)
    for k in range(top):
        hit = e_of == rt[k : k + 1, :]
        chosen = chosen + hit.astype(F32)
        gate = gate + jnp.where(hit, gt[k : k + 1, :], 0.0)
    place = slot_of(chosen, 1 - lane_ref[0], slots).T.astype(BF)
    gate = gate.T
    g1 = gate.astype(BF)
    rest = gate - g1.astype(F32)
    g2 = rest.astype(BF)
    g3 = (rest - g2.astype(F32)).astype(BF)
    n = slots * experts
    r = iota((1, n), 1)
    e_r = div_const(r, slots)
    slot = (r - e_r * slots).astype(F32)
    rep = bf(iota((experts, n), 0) == e_r)
    here = dot(place, rep) == slot
    for i, piece in enumerate((g1, g2, g3)):
        mix_ref[i * toks : (i + 1) * toks, :] = jnp.where(here, dot(piece, rep), 0.0).astype(BF)


def add_body(a_ref, b_ref, out_ref):
    total = a_ref[...].astype(F32) + b_ref[...].astype(F32)
    out_ref[...] = total.astype(BF).reshape(out_ref.shape)


def last_body(mix_ref, back_ref, out_ref):
    toks = out_ref.shape[0]
    s = dot(mix_ref[...], flat(back_ref))
    out_ref[...] = (s[:toks] + s[toks : 2 * toks] + s[2 * toks :]).astype(BF)


def per_device(tokens, routes, gates, norm_gain, w_gate, w_up, w_down):
    toks, width = tokens.shape
    top = routes.shape[1]
    experts = lax.axis_size("ep")
    cap = max(2, min(toks, 3 * toks * top // experts))
    slots = -(-cap // 4) * 2
    ff = w_gate.shape[2]
    items = experts * slots
    pairs = pltpu.VMEM((items // 2, 2, width), BF)
    tall = pltpu.VMEM((items, width), BF)
    swap = lambda v: lax.ppermute(v, "tp", [(0, 1), (1, 0)])
    lanes = lax.axis_index("tp").astype(jnp.int32).reshape(1)
    in_hbm = lambda *vs: [pltpu.with_memory_space_constraint(v, pltpu.HBM) for v in vs]
    wg, wu, wd = w_gate[0], w_up[0], w_down[0]

    outgoing, wu, mix = call(
        functools.partial(prep_body, experts=experts, slots=slots),
        (pairs, pltpu.VMEM(wu.shape, BF), pltpu.VMEM((3 * toks, items), BF)),
        [SMEM] + [HBM] * 5,
        [
            pltpu.VMEM((toks, width), BF),
            pltpu.VMEM((1, width), F32),
            pltpu.VMEM((top, toks), jnp.int32),
            pltpu.VMEM((top, toks), F32),
            pltpu.SemaphoreType.DMA((5,)),
        ],
        flops=2 * items * toks * width,
    )(lanes, *in_hbm(tokens, norm_gain.reshape(1, width), routes.T, gates.T, wu))
    exchange = lambda v: lax.all_to_all(
        v.reshape(experts, slots // 2, 2, width), "ep", split_axis=0, concat_axis=0, tiled=True
    ).reshape(v.shape)
    mine = exchange(outgoing)
    other = swap(mine)
    work = 2 * items * width * 3 * ff
    held = pltpu.VMEM((items, ff), BF)
    sent, wd = call(
        own_body, (tall, pltpu.VMEM(wd.shape, BF)), [VMEM] * 3 + [HBM],
        [held, pltpu.SemaphoreType.DMA((1,))], flops=work,
    )(mine, wg, wu, *in_hbm(wd))
    got = swap(sent)
    kept = call(other_body, tall, [VMEM] * 4, [held], flops=work)(other, wg, wu, wd)
    back = exchange(call(add_body, pairs, [VMEM] * 2, flops=items * width)(kept, got))
    part = call(
        last_body, pltpu.VMEM((toks, width), BF), [VMEM] * 2, flops=2 * 3 * toks * items * width
    )(mix, back)
    return (part.astype(F32) + swap(part).astype(F32)).astype(BF)


def solution(mesh):
    return jax.shard_map(
        per_device,
        mesh=mesh,
        in_specs=(
            P(("grp", "ep"), None),
            P(("grp", "ep"), None),
            P(("grp", "ep"), None),
            P(),
            P("ep", None, "tp"),
            P("ep", None, "tp"),
            P("ep", "tp", None),
        ),
        out_specs=P(("grp", "ep"), None),
        check_vma=False,
    )
```

```python
import functools

import jax
import jax.numpy as jnp
from jax import lax
from jax.experimental import pallas as pl
from jax.experimental.pallas import tpu as pltpu
from jax.sharding import PartitionSpec as P

EPS = 1e-06
BF = jnp.bfloat16
F32 = jnp.float32
VMEM = pl.BlockSpec(memory_space=pltpu.VMEM)
SMEM = pl.BlockSpec(memory_space=pltpu.SMEM)
HBM = pl.BlockSpec(memory_space=pltpu.HBM)
LIMIT = 16 * 1024 * 1024
PIECES = 8


def dot(a, b):
    return jnp.dot(a, b, preferred_element_type=F32)


def iota(shape, dim):
    return lax.broadcasted_iota(jnp.int32, shape, dim)


def div_const(x, n):
    return (x * (-(-(1 << 17) // n))) >> 17


def bf(mask):
    return jnp.where(mask, 1.0, 0.0).astype(BF)


def flat(ref):
    pairs, two, width = ref.shape
    return ref[...].reshape(pairs * two, width)


def call(body, outs, in_specs, scratch=(), flops=0):
    return pl.pallas_call(
        body,
        out_shape=outs,
        in_specs=in_specs,
        out_specs=jax.tree.map(lambda _: VMEM, outs),
        scratch_shapes=list(scratch),
        compiler_params=pltpu.CompilerParams(vmem_limit_bytes=LIMIT),
        cost_estimate=pl.CostEstimate(flops=flops, bytes_accessed=0, transcendentals=0),
    )


def start_all(pairs, sems):
    copies = [pltpu.make_async_copy(a, b, sems.at[i]) for i, (a, b) in enumerate(pairs)]
    for c in copies:
        c.start()
    return copies


def slot_of(chosen, core, slots):
    toks = chosen.shape[1]
    upper = bf(iota((toks, toks), 0) < iota((toks, toks), 1))
    rel = dot(chosen.astype(BF), upper) - (core * slots).astype(F32)
    return jnp.where((chosen > 0) & (rel >= 0) & (rel < slots), rel, -1.0)


def prep_body(
    lane_ref, tok_hbm, gain_hbm, rt_hbm, gt_hbm, wu_hbm,
    out_ref, wu_ref, mix_ref,
    tok_ref, gain_ref, rt_ref, gt_ref, sems, *, experts, slots,
):
    step = wu_ref.shape[0] // PIECES
    pieces = [slice(i * step, (i + 1) * step) for i in range(PIECES)]
    copies = start_all(
        ((rt_hbm, rt_ref), (tok_hbm, tok_ref), (gain_hbm, gain_ref), (gt_hbm, gt_ref))
        + tuple((wu_hbm.at[p], wu_ref.at[p]) for p in pieces),
        sems,
    )
    for c in copies[:4]:
        c.wait()
    toks = tok_ref.shape[0]
    xf = tok_ref[...].astype(F32)
    var = jnp.mean(xf * xf, axis=-1, keepdims=True)
    normed = (xf * lax.rsqrt(var + EPS) * gain_ref[...]).astype(BF)
    e_of = iota((experts, toks), 0)
    chosen = jnp.zeros((experts, toks), F32)
    for k in range(rt_ref.shape[0]):
        chosen = chosen + (e_of == rt_ref[k : k + 1, :]).astype(F32)
    place = slot_of(chosen, lane_ref[0], slots).astype(BF)
    n = slots * experts
    e_row = div_const(iota((n, experts), 0), slots)
    r = iota((n, toks), 0)
    slot = (r - div_const(r, slots) * slots).astype(F32)
    one = bf(dot(bf(iota((n, experts), 1) == e_row), place) == slot)
    out_ref[...] = dot(one, normed).astype(BF).reshape(out_ref.shape)
    table(lane_ref, rt_ref[...], gt_ref[...], mix_ref, slots, experts)
    for c in copies[4:]:
        c.wait()


def hidden_units(rows, wg_ref, wu_ref, hid_ref):
    for n in range(hid_ref.shape[1] // 128):
        cols = slice(n * 128, (n + 1) * 128)
        both = dot(rows, jnp.concatenate([wg_ref[:, cols], wu_ref[:, cols]], axis=1))
        g, u = both[:, :128], both[:, 128:]
        hid_ref[:, cols] = ((0.5 * g) * (1.0 + jnp.tanh(0.5 * g)) * u).astype(BF)


def own_body(x_ref, wg_ref, wu_ref, wd_hbm, out_ref, wd_ref, hid_ref, sems):
    (copy,) = start_all(((wd_hbm, wd_ref),), sems)
    hidden_units(flat(x_ref), wg_ref, wu_ref, hid_ref)
    copy.wait()
    out_ref[...] = dot(hid_ref[...], wd_ref[...]).astype(BF)


def other_body(x_ref, wg_ref, wu_ref, wd_ref, out_ref, hid_ref):
    hidden_units(flat(x_ref), wg_ref, wu_ref, hid_ref)
    out_ref[...] = dot(hid_ref[...], wd_ref[...]).astype(BF)


def table(lane_ref, rt, gt, mix_ref, slots, experts):
    top, toks = rt.shape
    e_of = iota((experts, toks), 0)
    chosen = jnp.zeros((experts, toks), F32)
    gate = jnp.zeros((experts, toks), F32)
    for k in range(top):
        hit = e_of == rt[k : k + 1, :]
        chosen = chosen + hit.astype(F32)
        gate = gate + jnp.where(hit, gt[k : k + 1, :], 0.0)
    place = slot_of(chosen, 1 - lane_ref[0], slots).T.astype(BF)
    gate = gate.T
    g1 = gate.astype(BF)
    rest = gate - g1.astype(F32)
    g2 = rest.astype(BF)
    g3 = (rest - g2.astype(F32)).astype(BF)
    n = slots * experts
    r = iota((1, n), 1)
    e_r = div_const(r, slots)
    slot = (r - e_r * slots).astype(F32)
    rep = bf(iota((experts, n), 0) == e_r)
    here = dot(place, rep) == slot
    for i, piece in enumerate((g1, g2, g3)):
        mix_ref[i * toks : (i + 1) * toks, :] = jnp.where(here, dot(piece, rep), 0.0).astype(BF)


def add_body(a_ref, b_ref, out_ref):
    total = a_ref[...].astype(F32) + b_ref[...].astype(F32)
    out_ref[...] = total.astype(BF).reshape(out_ref.shape)


def last_body(mix_ref, back_ref, out_ref):
    toks = out_ref.shape[0]
    s = dot(mix_ref[...], flat(back_ref))
    out_ref[...] = s[:toks] + s[toks : 2 * toks] + s[2 * toks :]


def per_device(tokens, routes, gates, norm_gain, w_gate, w_up, w_down):
    toks, width = tokens.shape
    top = routes.shape[1]
    experts = lax.axis_size("ep")
    cap = max(2, min(toks, 3 * toks * top // experts))
    slots = -(-cap // 4) * 2
    ff = w_gate.shape[2]
    items = experts * slots
    pairs = pltpu.VMEM((items // 2, 2, width), BF)
    tall = pltpu.VMEM((items, width), BF)
    swap = lambda v: lax.ppermute(v, "tp", [(0, 1), (1, 0)])
    lanes = lax.axis_index("tp").astype(jnp.int32).reshape(1)
    in_hbm = lambda *vs: [pltpu.with_memory_space_constraint(v, pltpu.HBM) for v in vs]
    wg, wu, wd = w_gate[0], w_up[0], w_down[0]

    outgoing, wu, mix = call(
        functools.partial(prep_body, experts=experts, slots=slots),
        (pairs, pltpu.VMEM(wu.shape, BF), pltpu.VMEM((3 * toks, items), BF)),
        [SMEM] + [HBM] * 5,
        [
            pltpu.VMEM((toks, width), BF),
            pltpu.VMEM((1, width), F32),
            pltpu.VMEM((top, toks), jnp.int32),
            pltpu.VMEM((top, toks), F32),
            pltpu.SemaphoreType.DMA((4 + PIECES,)),
        ],
        flops=2 * items * toks * width,
    )(lanes, *in_hbm(tokens, norm_gain.reshape(1, width), routes.T, gates.T, wu))
    exchange = lambda v: lax.all_to_all(
        v.reshape(experts, slots // 2, 2, width), "ep", split_axis=0, concat_axis=0, tiled=True
    ).reshape(v.shape)
    mine = exchange(outgoing)
    other = swap(mine)
    work = 2 * items * width * 3 * ff
    held = pltpu.VMEM((items, ff), BF)
    sent, wd = call(
        own_body, (tall, pltpu.VMEM(wd.shape, BF)), [VMEM] * 3 + [HBM],
        [held, pltpu.SemaphoreType.DMA((1,))], flops=work,
    )(mine, wg, wu, *in_hbm(wd))
    got = swap(sent)
    kept = call(other_body, tall, [VMEM] * 4, [held], flops=work)(other, wg, wu, wd)
    back = exchange(call(add_body, pairs, [VMEM] * 2, flops=items * width)(kept, got))
    part = call(
        last_body, pltpu.VMEM((toks, width), F32), [VMEM] * 2, flops=2 * 3 * toks * items * width
    )(mix, back)
    return (part + swap(part)).astype(BF)


def solution(mesh):
    return jax.shard_map(
        per_device,
        mesh=mesh,
        in_specs=(
            P(("grp", "ep"), None),
            P(("grp", "ep"), None),
            P(("grp", "ep"), None),
            P(),
            P("ep", None, "tp"),
            P("ep", None, "tp"),
            P("ep", "tp", None),
        ),
        out_specs=P(("grp", "ep"), None),
        check_vma=False,
    )
```

```python
import functools

import jax
import jax.numpy as jnp
from jax import lax
from jax.experimental import pallas as pl
from jax.experimental.pallas import tpu as pltpu
from jax.sharding import PartitionSpec as P

EPS = 1e-06
BF = jnp.bfloat16
F32 = jnp.float32
VMEM = pl.BlockSpec(memory_space=pltpu.VMEM)
SMEM = pl.BlockSpec(memory_space=pltpu.SMEM)
HBM = pl.BlockSpec(memory_space=pltpu.HBM)
LIMIT = 16 * 1024 * 1024
PIECES = 8


def dot(a, b):
    return jnp.dot(a, b, preferred_element_type=F32)


def iota(shape, dim):
    return lax.broadcasted_iota(jnp.int32, shape, dim)


def div_const(x, n):
    return (x * (-(-(1 << 17) // n))) >> 17


def bf(mask):
    return jnp.where(mask, 1.0, 0.0).astype(BF)


def flat(ref):
    pairs, two, width = ref.shape
    return ref[...].reshape(pairs * two, width)


def call(body, outs, in_specs, scratch=(), flops=0):
    return pl.pallas_call(
        body,
        out_shape=outs,
        in_specs=in_specs,
        out_specs=jax.tree.map(lambda _: VMEM, outs),
        scratch_shapes=list(scratch),
        compiler_params=pltpu.CompilerParams(vmem_limit_bytes=LIMIT),
        cost_estimate=pl.CostEstimate(flops=flops, bytes_accessed=0, transcendentals=0),
    )


def start_all(pairs, sems):
    copies = [pltpu.make_async_copy(a, b, sems.at[i]) for i, (a, b) in enumerate(pairs)]
    for c in copies:
        c.start()
    return copies


def slot_of(rank, core, slots):
    rel = rank - (core * slots).astype(F32)
    return jnp.where((rank >= 0) & (rel >= 0) & (rel < slots), rel, -1.0)


def prep_body(
    lane_ref, tok_hbm, gain_hbm, rt_hbm, gt_hbm, wu_hbm,
    out_ref, wu_ref, mix_ref,
    tok_ref, gain_ref, rt_ref, gt_ref, sems, *, experts, slots,
):
    step = wu_ref.shape[0] // PIECES
    pieces = [slice(i * step, (i + 1) * step) for i in range(PIECES)]
    few = tok_ref.shape[0] // 4
    blocks = [slice(i * few, (i + 1) * few) for i in range(4)]
    copies = start_all(
        ((rt_hbm, rt_ref), (gain_hbm, gain_ref), (gt_hbm, gt_ref))
        + tuple((tok_hbm.at[p], tok_ref.at[p]) for p in blocks)
        + tuple((wu_hbm.at[p], wu_ref.at[p]) for p in pieces),
        sems,
    )
    for c in copies[:7]:
        c.wait()
    toks = tok_ref.shape[0]
    xf = tok_ref[...].astype(F32)
    var = jnp.mean(xf * xf, axis=-1, keepdims=True)
    normed = (xf * lax.rsqrt(var + EPS) * gain_ref[...]).astype(BF)
    e_of = iota((experts, toks), 0)
    chosen = jnp.zeros((experts, toks), F32)
    gate = jnp.zeros((experts, toks), F32)
    for k in range(rt_ref.shape[0]):
        hit = e_of == rt_ref[k : k + 1, :]
        chosen = chosen + hit.astype(F32)
        gate = gate + jnp.where(hit, gt_ref[k : k + 1, :], 0.0)
    upper = bf(iota((toks, toks), 0) < iota((toks, toks), 1))
    rank = jnp.where(chosen > 0, dot(chosen.astype(BF), upper), -1.0)
    place = slot_of(rank, lane_ref[0], slots).astype(BF)
    n = slots * experts
    e_row = div_const(iota((n, experts), 0), slots)
    r = iota((n, toks), 0)
    slot = (r - div_const(r, slots) * slots).astype(F32)
    one = bf(dot(bf(iota((n, experts), 1) == e_row), place) == slot)
    out_ref[...] = dot(one, normed).astype(BF).reshape(out_ref.shape)
    table(slot_of(rank, 1 - lane_ref[0], slots).T.astype(BF), gate.T, mix_ref, slots)
    for c in copies[7:]:
        c.wait()


def hidden_units(rows, wg_ref, wu_ref, hid_ref):
    for n in range(hid_ref.shape[1] // 128):
        cols = slice(n * 128, (n + 1) * 128)
        both = dot(rows, jnp.concatenate([wg_ref[:, cols], wu_ref[:, cols]], axis=1))
        g, u = both[:, :128], both[:, 128:]
        hid_ref[:, cols] = ((0.5 * g) * (1.0 + jnp.tanh(0.5 * g)) * u).astype(BF)


def own_body(x_ref, wg_ref, wu_ref, wd_hbm, out_ref, wd_ref, hid_ref, sems):
    (copy,) = start_all(((wd_hbm, wd_ref),), sems)
    hidden_units(flat(x_ref), wg_ref, wu_ref, hid_ref)
    copy.wait()
    out_ref[...] = dot(hid_ref[...], wd_ref[...]).astype(BF)


def other_body(x_ref, wg_ref, wu_ref, wd_ref, out_ref, hid_ref):
    hidden_units(flat(x_ref), wg_ref, wu_ref, hid_ref)
    out_ref[...] = dot(hid_ref[...], wd_ref[...]).astype(BF)


def table(place, gate, mix_ref, slots):
    toks, experts = gate.shape
    g1 = gate.astype(BF)
    rest = gate - g1.astype(F32)
    g2 = rest.astype(BF)
    g3 = (rest - g2.astype(F32)).astype(BF)
    n = slots * experts
    r = iota((1, n), 1)
    e_r = div_const(r, slots)
    slot = (r - e_r * slots).astype(F32)
    rep = bf(iota((experts, n), 0) == e_r)
    spread = dot(jnp.concatenate([place, g1, g2, g3], axis=0), rep)
    here = spread[:toks] == slot
    for i in range(3):
        piece = spread[(i + 1) * toks : (i + 2) * toks]
        mix_ref[i * toks : (i + 1) * toks, :] = jnp.where(here, piece, 0.0).astype(BF)


def add_body(a_ref, b_ref, out_ref):
    total = a_ref[...].astype(F32) + b_ref[...].astype(F32)
    out_ref[...] = total.astype(BF).reshape(out_ref.shape)


def last_body(mix_ref, back_ref, out_ref):
    toks = out_ref.shape[0]
    s = dot(mix_ref[...], flat(back_ref))
    out_ref[...] = s[:toks] + s[toks : 2 * toks] + s[2 * toks :]


def per_device(tokens, routes, gates, norm_gain, w_gate, w_up, w_down):
    toks, width = tokens.shape
    top = routes.shape[1]
    experts = lax.axis_size("ep")
    cap = max(2, min(toks, 3 * toks * top // experts))
    slots = -(-cap // 4) * 2
    ff = w_gate.shape[2]
    items = experts * slots
    pairs = pltpu.VMEM((items // 2, 2, width), BF)
    tall = pltpu.VMEM((items, width), BF)
    swap = lambda v: lax.ppermute(v, "tp", [(0, 1), (1, 0)])
    lanes = lax.axis_index("tp").astype(jnp.int32).reshape(1)
    in_hbm = lambda *vs: [pltpu.with_memory_space_constraint(v, pltpu.HBM) for v in vs]
    wg, wu, wd = w_gate[0], w_up[0], w_down[0]

    outgoing, wu, mix = call(
        functools.partial(prep_body, experts=experts, slots=slots),
        (pairs, pltpu.VMEM(wu.shape, BF), pltpu.VMEM((3 * toks, items), BF)),
        [SMEM] + [HBM] * 5,
        [
            pltpu.VMEM((toks, width), BF),
            pltpu.VMEM((1, width), F32),
            pltpu.VMEM((top, toks), jnp.int32),
            pltpu.VMEM((top, toks), F32),
            pltpu.SemaphoreType.DMA((7 + PIECES,)),
        ],
        flops=2 * items * toks * width,
    )(lanes, *in_hbm(tokens, norm_gain.reshape(1, width), routes.T, gates.T, wu))
    exchange = lambda v: lax.all_to_all(
        v.reshape(experts, slots // 2, 2, width), "ep", split_axis=0, concat_axis=0, tiled=True
    ).reshape(v.shape)
    mine = exchange(outgoing)
    other = swap(mine)
    work = 2 * items * width * 3 * ff
    held = pltpu.VMEM((items, ff), BF)
    sent, wd = call(
        own_body, (tall, pltpu.VMEM(wd.shape, BF)), [VMEM] * 3 + [HBM],
        [held, pltpu.SemaphoreType.DMA((1,))], flops=work,
    )(mine, wg, wu, *in_hbm(wd))
    got = swap(sent)
    kept = call(other_body, tall, [VMEM] * 4, [held], flops=work)(other, wg, wu, wd)
    back = exchange(call(add_body, pairs, [VMEM] * 2, flops=items * width)(kept, got))
    part = call(
        last_body, pltpu.VMEM((toks, width), F32), [VMEM] * 2, flops=2 * 3 * toks * items * width
    )(mix, back)
    return (part + swap(part)).astype(BF)


def solution(mesh):
    return jax.shard_map(
        per_device,
        mesh=mesh,
        in_specs=(
            P(("grp", "ep"), None),
            P(("grp", "ep"), None),
            P(("grp", "ep"), None),
            P(),
            P("ep", None, "tp"),
            P("ep", None, "tp"),
            P("ep", "tp", None),
        ),
        out_specs=P(("grp", "ep"), None),
        check_vma=False,
    )
```
